512 devices in a mesh: grp: 2 (over y), sp: 16 (over z), dp: 16 (over x, core).
Axes of the slice: x: 8, y: 2, z: 16, core: 2. Of those that a mesh axis runs over, the one named last changes fastest.
The devices are a block of a 8x8x16 slice.
Arguments:
- gate_input: bfloat16 [32, 6144, 2048], P(('grp', 'dp'), 'sp'), parts along dimension 0, may hold values from -6 to 6
- value_input: bfloat16 [32, 6144, 2048], P(('grp', 'dp'), 'sp'), parts along dimension 0, may hold values from -6 to 6
- norm_gain: bfloat16 [2048], replicated, may hold values from 0.099609375 to 1.8984375
- norm_bias: bfloat16 [2048], replicated, may hold values from -2.5 to 2.5
- mix_weight: bfloat16 [16, 1024, 1024], P('sp', 'dp'), may hold values from -0.1875 to 0.1875
- mix_bias: bfloat16 [16, 1024], P('sp'), may hold values from 0.099609375 to 1.8984375
Outputs:
- gated: bfloat16 [32, 6144, 2048], P(('grp', 'dp'), 'sp'), parts along dimension 0
The draws below stay inside these ranges and needn't reach their ends.
There are 2 independent parts, one for each index of `grp`. The reference program is written for one: setup_inputs(seed, part) draws one part's arguments, and reference() takes and returns one part's arrays. A program takes and returns all parts, laid end to end along the dimension named above; an argument that names none is the same for every part. Nothing has to cross between parts.
All inputs are finite; a program needn't handle non-finite values.
Results may differ from the reference program's by a relative error of at most 0.0053.
Values may be sent and summed in bfloat16 or wider, within the bound.
A program may use at most 64 MiB of HBM per device.

```python
import jax
import jax.numpy as jnp
from jax import lax

GD = 128
G = 16
GW = 2048
BLK = 1024
LEN = 6144
SEQS = 16


def level_of(rng, dims, cuts, low, top_value):
    gain = 1.0
    for position, shards_of in cuts:
        draws = jax.random.uniform(jax.random.fold_in(jax.random.fold_in(rng, 6), position), (shards_of,), jnp.float32, low / len(cuts), top_value / len(cuts))
        gain = gain * jnp.repeat(jnp.exp(draws), dims[position] // shards_of).reshape((-1,) + (1,) * (len(dims) - 1 - position))
    return gain


def gaussian(stream_key, dims, deviation, limit, pieces=(), held_as=jnp.bfloat16):
    values = deviation * jax.random.normal(stream_key, dims, jnp.float32)
    if pieces:
        values = values * level_of(stream_key, dims, pieces, -0.22, 0.18)
    return jnp.clip(values, -limit, limit).astype(held_as)


def setup_inputs(seed: int = 0, part: int = 0) -> dict:
    key_of = jax.random.split(jax.random.key(seed), 7)
    part_keys = jax.random.split(jax.random.fold_in(key_of[6], part), 7)
    gate_input = gaussian(part_keys[0], (SEQS, LEN, GW), 1.0, 6.0, ((0, 16), (1, 16)))
    value_input = gaussian(part_keys[1], (SEQS, LEN, GW), 1.0, 6.0, ((0, 16), (1, 16)))
    norm_gain = jnp.clip(1.0 + 0.18 * jax.random.normal(key_of[2], (GW,), jnp.float32), 0.099609375, 1.8984375).astype(jnp.bfloat16)
    norm_bias = gaussian(key_of[3], (GW,), 0.5, 2.5)
    mix_weight = gaussian(key_of[4], (G, BLK, BLK), BLK ** -0.5, 0.1875, ((0, 16), (1, 16)))
    mix_bias = jnp.clip(1.0 + 0.18 * jax.random.normal(key_of[5], (G, BLK), jnp.float32), 0.099609375, 1.8984375).astype(jnp.bfloat16)
    return {"gate_input": gate_input, "value_input": value_input, "norm_gain": norm_gain, "norm_bias": norm_bias, "mix_weight": mix_weight, "mix_bias": mix_bias}


def reference(gate_input, value_input, norm_gain, norm_bias, mix_weight, mix_bias):
    seqs, length, width = value_input.shape
    nblocks = -(-length // BLK)
    act = jax.nn.gelu(value_input.astype(jnp.float32))
    mean = lax.optimization_barrier(jnp.mean(act, axis=-1, keepdims=True))
    var = lax.optimization_barrier(jnp.mean(jnp.square(act - mean), axis=-1, keepdims=True))
    normed = ((act - mean) * lax.rsqrt(var + 1e-06) * norm_gain.astype(jnp.float32) + norm_bias.astype(jnp.float32)).astype(jnp.bfloat16)
    keep = jnp.tril(jnp.ones((BLK, BLK), dtype=bool))
    weight_full = jnp.where(keep[None], mix_weight.astype(jnp.float32), jnp.float32(0.0))
    bias_full = mix_bias.astype(jnp.float32).T[None, :, :, None]

    def mix_sequence(normed_seq):
        padded = jnp.pad(normed_seq, ((0, nblocks * BLK - length), (0, 0)))
        blocks = padded.reshape(nblocks, BLK, G, GD).astype(jnp.float32)
        mixed = jnp.einsum('gts,bsgc->btgc', weight_full, blocks) + bias_full
        return mixed.reshape(nblocks * BLK, width)[:length].astype(jnp.bfloat16)
    mixed = lax.map(mix_sequence, normed)
    mixed = lax.optimization_barrier(mixed)
    gated = jax.nn.gelu(gate_input.astype(jnp.float32)) * mixed.astype(jnp.float32)
    return gated.astype(jnp.bfloat16)
```

```python
import functools

import jax
import jax.numpy as jnp
from jax import lax
from jax.experimental import pallas as pl
from jax.experimental.pallas import tpu as pltpu
from jax.sharding import PartitionSpec as P

GD = 128
BLK = 1024
MESH = pl.DeviceIdType.MESH


class Plan:
    def __init__(self, sp, dp, length, width, rows, blk):
        self.sp, self.dp = sp, dp
        self.X = dp // 2
        self.C = rows * 2
        self.R = blk // self.C
        self.NI = length // self.C
        self.NB = sp * length // blk
        self.G = width // GD
        self.S = self.NB * self.G // sp
        self.SH = self.S // 2
        self.T = self.C // self.X
        self.PR = self.R // 2
        self.PW = self.C * (self.R + 1)
        self.HALF = self.X // 2
        far = 0
        for z in range(sp):
            for i in range(self.NI):
                for u in range(self.G):
                    far = max(far, abs((self.G * ((self.NI * z + i) // self.R) + u) // self.S - z))
        self.far = far

    def turn(self, b):
        return (self.G // 2 + self.G - (self.G * b + self.G // 2) // self.S) % self.G

    def group(self, p):
        b = p // self.G
        return b, (p % self.G + self.G - self.turn(b)) % self.G

    def item(self, b, g):
        return self.G * b + (g + self.turn(b)) % self.G


def loop(n, body):
    def step(k, carry):
        body(k)
        return carry

    lax.fori_loop(0, n, step, 0)


def mixer(plan, w, bias, normed, out, wbuf, xin, y, bbuf, w1s, w1r, bs, br, xs, xr, rs, rr, rl, ps, pr, ys, yr):
    X, C, R, NI, NB, G, S, SH, T, PR = (
        plan.X, plan.C, plan.R, plan.NI, plan.NB, plan.G, plan.S, plan.SH, plan.T, plan.PR,
    )
    z = lax.axis_index("sp")
    d = lax.axis_index("dp")
    x, c = d // 2, d % 2
    right = {"sp": z, "dp": 2 * ((x + 1) % X) + c}
    left = {"sp": z, "dp": 2 * ((x + X - 1) % X) + c}
    partner = {"sp": z, "dp": 2 * x + 1 - c}

    def remote(src, dst, send, recv, to):
        return pltpu.make_async_remote_copy(
            src_ref=src, dst_ref=dst, send_sem=send, recv_sem=recv, device_id=to, device_id_type=MESH
        )

    def put(src, dst, send, recv, sp, dp):
        here = jnp.logical_and(sp == z, dp == d)

        @pl.when(here)
        def _():
            pltpu.make_async_copy(src, dst, recv).start()

        @pl.when(jnp.logical_not(here))
        def _():
            remote(src, dst, send, recv, {"sp": sp, "dp": dp}).start()

    def arrived(ref, sem):
        pltpu.make_async_copy(ref, ref, sem).wait()

    bar = pltpu.get_barrier_semaphore()

    def greet(sp, dp):
        apart = jnp.logical_or(sp != z, dp != d)

        @pl.when(apart)
        def _():
            pl.semaphore_signal(bar, inc=1, device_id={"sp": sp, "dp": dp}, device_id_type=MESH)

        return apart.astype(jnp.int32)

    def greet_sources(jj, met):
        _, g = plan.group(S * z + SH * c + jj)
        return lax.fori_loop(0, X, lambda k, n: n + greet(g, 2 * k + x // plan.HALF), met)

    met = lax.fori_loop(0, SH, greet_sources, jnp.int32(0))
    met = lax.fori_loop(0, S, lambda j, n: n + greet(plan.group(S * z + j)[1], d), met)
    for far in range(1, plan.far + 1):
        greet((z + far) % plan.sp, d)
        greet((z + plan.sp - far) % plan.sp, d)
    for to in (right, left, partner):
        pl.semaphore_signal(bar, inc=1, device_id=to, device_id_type=MESH)
    pl.semaphore_wait(bar, met + 2 * plan.far + 3)

    def first_leg(k, act):
        ncol = C * (k + 1)
        row = min(k, R - 1 - k) * T
        col = 0 if k < R // 2 else C * (R - k)

        def one(jj, b):
            p = plan.item(b, z)
            j, own = p % S, p // S

            @pl.when(j % SH == jj)
            def _():
                def strip(q):
                    xp = plan.HALF * c + q
                    act(
                        w.at[pl.ds(pl.multiple_of(q * T, T), T), pl.ds(0, ncol)],
                        wbuf.at[j, xp, pl.ds(row, T), pl.ds(col, ncol)],
                        w1r.at[jj], own, 2 * xp + j // SH,
                    )

                loop(plan.HALF, strip)

        loop(SH, lambda jj: loop(NB, lambda b: one(jj, b)))

    for k in range(X):
        @pl.when(x == k)
        def _(k=k):
            first_leg(k, lambda src, dst, recv, sp, dp: put(src, dst, w1s, recv, sp, dp))

    def send_bias(b):
        p = plan.item(b, z)
        put(bias, bbuf.at[p % S], bs, br, p // S, d)

    loop(NB, send_bias)

    per = -(-G // SH)

    def unit(jj, i, t, act):
        ch = NI * z + i
        b, r = ch // R, ch % R
        u = (jj + G * SH * NB - G * b) % SH + SH * t

        @pl.when(u < G)
        def _():
            p = G * b + u
            act(i, r, plan.group(p)[1], p)

    def send_unit(i, r, g, p):
        src = normed.at[pl.ds(pl.multiple_of(i * C, C), C), pl.ds(pl.multiple_of(g * GD, GD), GD)]
        put(src, xin.at[p % S, r], xs, xr.at[p % S], p // S, d)

    loop(SH, lambda jj: loop(NI, lambda i: loop(per, lambda t: unit(jj, i, t, send_unit))))

    hops = plan.HALF

    def pass_on(jj, blk, send, recv, to):
        remote(wbuf.at[SH * c + jj, blk], wbuf.at[SH * c + jj, blk], send, recv, to).start()

    def ring(jj, s):
        more = (jj + c) % 2 == 0
        if s == 0:
            arrived(wbuf.at[SH * c + jj, x], w1r.at[jj])
            blk = x
            if X - hops - 1 >= 1:
                pass_on(jj, blk, rs, rr.at[jj, 0], right)
                pass_on(jj, blk, rs, rl.at[jj, 0], left)
            else:
                @pl.when(more)
                def _():
                    pass_on(jj, blk, rs, rr.at[jj, 0], right)

                @pl.when(jnp.logical_not(more))
                def _():
                    pass_on(jj, blk, rs, rl.at[jj, 0], left)
            pass_on(jj, blk, ps, pr.at[jj], partner)
            return
        for sems, to, blk, longer in (
            (rr, right, (x + X - s) % X, more),
            (rl, left, (x + s) % X, jnp.logical_not(more)),
        ):
            def step(forward, sems=sems, to=to, blk=blk):
                arrived(wbuf.at[SH * c + jj, blk], sems.at[jj, s - 1])
                if forward is True:
                    pass_on(jj, blk, rs, sems.at[jj, s], to)
                elif forward is not False:
                    @pl.when(forward)
                    def _():
                        pass_on(jj, blk, rs, sems.at[jj, s], to)
                pass_on(jj, blk, ps, pr.at[jj], partner)

            if s < hops - 1:
                step(True)
            elif s < hops:
                step(longer)
            else:
                pl.when(longer)(functools.partial(step, False))

    def compute(jj, other):
        co = jnp.where(other == 1, 1 - c, c)
        j = SH * co + jj
        b, g = plan.group(S * z + j)
        arrived(xin.at[j], xr.at[j])
        bcol = jnp.transpose(bbuf[j])
        keep = lax.broadcasted_iota(jnp.int32, (C, C), 1) <= lax.broadcasted_iota(jnp.int32, (C, C), 0)
        for r in range(R):
            row = min(r, R - 1 - r) * T
            col = 0 if r < R // 2 else C * (R - r)
            diag = wbuf[j, :, row : row + T, col + C * r : col + C * (r + 1)].reshape(C, C)
            diag = jnp.where(keep, diag, jnp.zeros_like(diag))
            acc = jnp.dot(diag, xin[j, r], preferred_element_type=jnp.float32)
            if r:
                before = wbuf[j, :, row : row + T, col : col + C * r].reshape(C, C * r)
                acc += jnp.dot(before, xin[j, :r].reshape(C * r, GD), preferred_element_type=jnp.float32)
            y[j, r] = (acc + bcol[:, r : r + 1]).astype(y.dtype)

        def give(r):
            ch = R * b + r
            sp, i = ch // NI, ch % NI
            dst = out.at[pl.ds(pl.multiple_of(i * C, C), C), pl.ds(pl.multiple_of(g * GD, GD), GD)]
            put(y.at[j, r], dst, ys, yr, sp, d)

        loop(R, give)

    last = hops
    events = sorted((s + jj, jj, s) for jj in range(SH) for s in range(last + 1))
    first = True
    for _, jj, s in events:
        ring(jj, s)
        if s == last:
            arrived(wbuf.at[SH * (1 - c) + jj], pr.at[jj])
            if first:
                arrived(bbuf, br)
                first = False
            loop(2, functools.partial(compute, jj))

    arrived(out, yr)

    for k in range(X):
        @pl.when(x == k)
        def _(k=k):
            def gone(src, dst, recv, sp, dp):
                @pl.when(jnp.logical_not(jnp.logical_and(sp == z, dp == d)))
                def _():
                    remote(src, dst, w1s, recv, {"sp": sp, "dp": dp}).wait_send()

            first_leg(k, gone)

    def bias_gone(b):
        p = plan.item(b, z)

        @pl.when(p // S != z)
        def _():
            remote(bias, bbuf.at[p % S], bs, br, {"sp": p // S, "dp": d}).wait_send()

    loop(NB, bias_gone)

    def unit_gone(i, r, g, p):
        @pl.when(p // S != z)
        def _():
            arrived(xin.at[0, 0], xs)

    loop(SH, lambda jj: loop(NI, lambda i: loop(per, lambda t: unit(jj, i, t, unit_gone))))

    def y_gone(j):
        b, _ = plan.group(S * z + j)

        def one(r):
            @pl.when((R * b + r) // NI != z)
            def _():
                arrived(y.at[0, 0], ys)

        loop(R, one)

    loop(S, y_gone)
    loop(SH * (X - 1), lambda k: arrived(wbuf.at[0, 0], rs))
    loop(SH * X, lambda k: arrived(wbuf.at[0, 0], ps))


def mix(plan, normed, w, bias):
    hop = max(plan.HALF, 1)
    dma = pltpu.SemaphoreType.DMA
    return pl.pallas_call(
        functools.partial(mixer, plan),
        out_shape=jax.ShapeDtypeStruct(normed.shape, normed.dtype),
        in_specs=[pl.BlockSpec(memory_space=pl.ANY)] * 3,
        out_specs=pl.BlockSpec(memory_space=pl.ANY),
        scratch_shapes=[
            pltpu.VMEM((plan.S, plan.X, plan.PR * plan.T, plan.PW), jnp.bfloat16),
            pltpu.VMEM((plan.S, plan.R, plan.C, GD), jnp.bfloat16),
            pltpu.VMEM((plan.S, plan.R, plan.C, GD), jnp.bfloat16),
            pltpu.VMEM((plan.S, plan.R, plan.C), jnp.float32),
            dma, dma((plan.SH,)), dma, dma, dma, dma((plan.S,)), dma,
            dma((plan.SH, hop)), dma((plan.SH, hop)), dma, dma((plan.SH,)), dma, dma,
        ],
        compiler_params=pltpu.CompilerParams(
            collective_id=0, has_side_effects=True, vmem_limit_bytes=40 * 1024 * 1024
        ),
    )(w, bias, normed)


def body(sp, dp, gate_input, value_input, norm_gain, norm_bias, mix_weight, mix_bias):
    length, width = value_input.shape[1:]
    rows, blk = mix_weight.shape[1:]
    plan = Plan(sp, dp, length, width, rows, blk)
    act = jax.nn.gelu(value_input[0].astype(jnp.float32))
    mean = jnp.mean(act, axis=-1, keepdims=True)
    var = jnp.mean(jnp.square(act - mean), axis=-1, keepdims=True)
    normed = (
        (act - mean) * lax.rsqrt(var + 1e-06) * norm_gain.astype(jnp.float32)
        + norm_bias.astype(jnp.float32)
    ).astype(jnp.bfloat16)
    bias = mix_bias[0].astype(jnp.float32).reshape(plan.R, plan.C)
    mixed = mix(plan, normed, mix_weight[0], bias)
    gated = jax.nn.gelu(gate_input.astype(jnp.float32)) * mixed[None].astype(jnp.float32)
    return gated.astype(jnp.bfloat16)


def solution(mesh):
    placed = (
        P(("grp", "dp"), "sp", None),
        P(("grp", "dp"), "sp", None),
        P(),
        P(),
        P("sp", "dp", None),
        P("sp", None),
    )
    return jax.shard_map(
        functools.partial(body, mesh.shape["sp"], mesh.shape["dp"]),
        mesh=mesh, in_specs=placed, out_specs=P(("grp", "dp"), "sp", None), check_vma=False,
    )
```

```python
import functools

import jax
import jax.numpy as jnp
from jax import lax
from jax.experimental import pallas as pl
from jax.experimental.pallas import tpu as pltpu
from jax.sharding import PartitionSpec as P

GD = 128
BLK = 1024
MESH = pl.DeviceIdType.MESH


class Plan:
    def __init__(self, sp, dp, length, width, rows, blk):
        self.sp, self.dp = sp, dp
        self.X = dp // 2
        self.C = rows * 2
        self.R = blk // self.C
        self.NI = length // self.C
        self.NB = sp * length // blk
        self.G = width // GD
        self.S = self.NB * self.G // sp
        self.SH = self.S // 2
        self.T = self.C // self.X
        self.PR = self.R // 2
        self.PW = self.C * (self.R + 1)
        self.HALF = self.X // 2
        far = 0
        for z in range(sp):
            for i in range(self.NI):
                for u in range(self.G):
                    far = max(far, abs((self.G * ((self.NI * z + i) // self.R) + u) // self.S - z))
        self.far = far

    def turn(self, b):
        return (self.G // 2 + self.G - (self.G * b + self.G // 2) // self.S) % self.G

    def group(self, p):
        b = p // self.G
        return b, (p % self.G + self.G - self.turn(b)) % self.G

    def item(self, b, g):
        return self.G * b + (g + self.turn(b)) % self.G


def loop(n, body):
    def step(k, carry):
        body(k)
        return carry

    lax.fori_loop(0, n, step, 0)


def mixer(plan, w, bias, value, gain, shift, out, normed, vbuf, nbuf, wbuf, xin, y, bbuf, vs, ns, w1s, w1r, bs, br, xs, xr, rs, rr, rl, ps, pr, ys, yr):
    X, C, R, NI, NB, G, S, SH, T, PR = (
        plan.X, plan.C, plan.R, plan.NI, plan.NB, plan.G, plan.S, plan.SH, plan.T, plan.PR,
    )
    z = lax.axis_index("sp")
    d = lax.axis_index("dp")
    x, c = d // 2, d % 2
    right = {"sp": z, "dp": 2 * ((x + 1) % X) + c}
    left = {"sp": z, "dp": 2 * ((x + X - 1) % X) + c}
    partner = {"sp": z, "dp": 2 * x + 1 - c}

    def remote(src, dst, send, recv, to):
        return pltpu.make_async_remote_copy(
            src_ref=src, dst_ref=dst, send_sem=send, recv_sem=recv, device_id=to, device_id_type=MESH
        )

    def put(src, dst, send, recv, sp, dp):
        here = jnp.logical_and(sp == z, dp == d)

        @pl.when(here)
        def _():
            pltpu.make_async_copy(src, dst, recv).start()

        @pl.when(jnp.logical_not(here))
        def _():
            remote(src, dst, send, recv, {"sp": sp, "dp": dp}).start()

    def arrived(ref, sem):
        pltpu.make_async_copy(ref, ref, sem).wait()

    def rows(k):
        return pl.ds(pl.multiple_of(k * C, C), C)

    load = pltpu.make_async_copy(value, vbuf, vs)
    load.start()

    bar = pltpu.get_barrier_semaphore()

    def greet(sp, dp):
        apart = jnp.logical_or(sp != z, dp != d)

        @pl.when(apart)
        def _():
            pl.semaphore_signal(bar, inc=1, device_id={"sp": sp, "dp": dp}, device_id_type=MESH)

        return apart.astype(jnp.int32)

    def greet_sources(jj, met):
        _, g = plan.group(S * z + SH * c + jj)
        return lax.fori_loop(0, X, lambda k, n: n + greet(g, 2 * k + x // plan.HALF), met)

    met = lax.fori_loop(0, SH, greet_sources, jnp.int32(0))
    met = lax.fori_loop(0, S, lambda j, n: n + greet(plan.group(S * z + j)[1], d), met)
    for far in range(1, plan.far + 1):
        greet((z + far) % plan.sp, d)
        greet((z + plan.sp - far) % plan.sp, d)
    for to in (right, left, partner):
        pl.semaphore_signal(bar, inc=1, device_id=to, device_id_type=MESH)
    with jax.named_scope("barrier"):
        pl.semaphore_wait(bar, met + 2 * plan.far + 3)

    def first_leg(k):
        ncol = C * (k + 1)
        row = min(k, R - 1 - k) * T
        col = 0 if k < R // 2 else C * (R - k)

        def one(jj, b):
            p = plan.item(b, z)
            j, own = p % S, p // S

            @pl.when(j % SH == jj)
            def _():
                def strip(q):
                    xp = plan.HALF * c + q
                    put(
                        w.at[pl.ds(pl.multiple_of(q * T, T), T), pl.ds(0, ncol)],
                        wbuf.at[j, xp, pl.ds(row, T), pl.ds(col, ncol)],
                        w1s, w1r.at[jj], own, 2 * xp + j // SH,
                    )

                loop(plan.HALF, strip)

        loop(SH, lambda jj: loop(NB, lambda b: one(jj, b)))

    def first_leg_gone():
        def kept(b, n):
            p = plan.item(b, z)
            return n + jnp.logical_and(p // S == z, p % S // SH == c).astype(jnp.int32)

        own = lax.fori_loop(0, NB, kept, jnp.int32(0)) * (x // plan.HALF == c).astype(jnp.int32)
        for k in range(X):
            @pl.when(x == k)
            def _(k=k):
                part = w.at[pl.ds(0, T), pl.ds(0, C * (k + 1))]
                loop(NB * plan.HALF - own, lambda _: arrived(part, w1s))

        def one(b):
            @pl.when(plan.item(b, z) // S != z)
            def _():
                arrived(bias, bs)

        loop(NB, one)

    with jax.named_scope("leg1_send"):
        for k in range(X):
            pl.when(x == k)(functools.partial(first_leg, k))

    def send_bias(b):
        p = plan.item(b, z)
        put(bias, bbuf.at[p % S], bs, br, p // S, d)

    loop(NB, send_bias)

    step_rows = min(16, C)

    def normalize(k):
        at = pl.ds(pl.multiple_of(k * step_rows, step_rows), step_rows)
        act = jax.nn.gelu(vbuf[at, :].astype(jnp.float32))
        mean = jnp.mean(act, axis=-1, keepdims=True)
        act = act - mean
        var = jnp.mean(jnp.square(act), axis=-1, keepdims=True)
        nbuf[at, :] = (act * lax.rsqrt(var + 1e-06) * gain[...] + shift[...]).astype(nbuf.dtype)

    with jax.named_scope("normalize"):
        load.wait()
        for i in range(NI):
            loop(C // step_rows, lambda k, i=i: normalize(i * (C // step_rows) + k))
            pltpu.make_async_copy(nbuf.at[rows(i)], normed.at[rows(i)], ns.at[i]).start()
        for i in range(NI):
            arrived(nbuf.at[rows(i)], ns.at[i])

    per = -(-G // SH)

    def send_units(jj, n):
        def unit(k, n):
            i, t = k // per, k % per
            ch = NI * z + i
            b, r = ch // R, ch % R
            u = (jj + G * SH * NB - G * b) % SH + SH * t
            p = G * b + u

            @pl.when(u < G)
            def _():
                g = plan.group(p)[1]
                src = normed.at[rows(i), pl.ds(pl.multiple_of(g * GD, GD), GD)]
                put(src, xin.at[p % S, r], xs, xr.at[p % S], p // S, d)

            return n + jnp.logical_and(u < G, p // S != z).astype(jnp.int32)

        with jax.named_scope(f"units{jj}"):
            return lax.fori_loop(0, NI * per, unit, n)

    hops = plan.HALF

    def pass_on(jj, blk, send, recv, to):
        remote(wbuf.at[SH * c + jj, blk], wbuf.at[SH * c + jj, blk], send, recv, to).start()

    def ring(jj, s):
        more = (jj + c) % 2 == 0
        if s == 0:
            arrived(wbuf.at[SH * c + jj, x], w1r.at[jj])
            blk = x
            if X - hops - 1 >= 1:
                pass_on(jj, blk, rs, rr.at[jj, 0], right)
                pass_on(jj, blk, rs, rl.at[jj, 0], left)
            else:
                @pl.when(more)
                def _():
                    pass_on(jj, blk, rs, rr.at[jj, 0], right)

                @pl.when(jnp.logical_not(more))
                def _():
                    pass_on(jj, blk, rs, rl.at[jj, 0], left)
            pass_on(jj, blk, ps, pr.at[jj], partner)
            return
        for sems, to, blk, longer in (
            (rr, right, (x + X - s) % X, more),
            (rl, left, (x + s) % X, jnp.logical_not(more)),
        ):
            def step(forward, sems=sems, to=to, blk=blk):
                arrived(wbuf.at[SH * c + jj, blk], sems.at[jj, s - 1])
                if forward is True:
                    pass_on(jj, blk, rs, sems.at[jj, s], to)
                elif forward is not False:
                    @pl.when(forward)
                    def _():
                        pass_on(jj, blk, rs, sems.at[jj, s], to)
                pass_on(jj, blk, ps, pr.at[jj], partner)

            if s < hops - 1:
                step(True)
            elif s < hops:
                step(longer)
            else:
                pl.when(longer)(functools.partial(step, False))

    def compute(jj, other):
        co = jnp.where(other == 1, 1 - c, c)
        j = SH * co + jj
        b, g = plan.group(S * z + j)
        arrived(xin.at[j], xr.at[j])
        bcol = jnp.transpose(bbuf[j])
        keep = lax.broadcasted_iota(jnp.int32, (C, C), 1) <= lax.broadcasted_iota(jnp.int32, (C, C), 0)
        for r in range(R):
            row = min(r, R - 1 - r) * T
            col = 0 if r < R // 2 else C * (R - r)
            diag = wbuf[j, :, row : row + T, col + C * r : col + C * (r + 1)].reshape(C, C)
            diag = jnp.where(keep, diag, jnp.zeros_like(diag))
            acc = jnp.dot(diag, xin[j, r], preferred_element_type=jnp.float32)
            if r:
                before = wbuf[j, :, row : row + T, col : col + C * r].reshape(C, C * r)
                acc += jnp.dot(before, xin[j, :r].reshape(C * r, GD), preferred_element_type=jnp.float32)
            y[j, r] = (acc + bcol[:, r : r + 1]).astype(y.dtype)

        def give(r):
            ch = R * b + r
            sp, i = ch // NI, ch % NI
            dst = out.at[pl.ds(pl.multiple_of(i * C, C), C), pl.ds(pl.multiple_of(g * GD, GD), GD)]
            put(y.at[j, r], dst, ys, yr, sp, d)

        loop(R, give)

    last = hops
    order = sorted((s + jj, jj, s) for jj in range(SH) for s in range(last + 1))
    order = [(jj, s) for _, jj, s in order]
    sent = jnp.int32(0)
    pending = []
    for n, (jj, s) in enumerate(order):
        with jax.named_scope(f"ring{jj}_{s}"):
            ring(jj, s)
        if s == 0:
            sent = send_units(jj, sent)
        if (jj, s) == order[-SH - 2]:
            with jax.named_scope("leg1_gone"):
                first_leg_gone()
        if s == last:
            pending.append(jj)
        if jj == SH - 1:
            for jj in pending:
                with jax.named_scope(f"partner{jj}"):
                    arrived(wbuf.at[SH * (1 - c) + jj], pr.at[jj])
                    if jj == 0:
                        arrived(bbuf, br)
                with jax.named_scope(f"compute{jj}"):
                    loop(2, functools.partial(compute, jj))
            pending = []
    with jax.named_scope("sends_gone"):
        loop(sent, lambda _: arrived(xin.at[0, 0], xs))
        loop(SH * (X - 1), lambda k: arrived(wbuf.at[0, 0], rs))
        loop(SH * X, lambda k: arrived(wbuf.at[0, 0], ps))
    with jax.named_scope("out_wait"):
        arrived(out, yr)
    with jax.named_scope("drain"):
        loop(sent, lambda _: arrived(y.at[0, 0], ys))


def mix(plan, value, gain, shift, w, bias):
    hop = max(plan.HALF, 1)
    dma = pltpu.SemaphoreType.DMA
    anywhere, vmem = pl.BlockSpec(memory_space=pl.ANY), pl.BlockSpec(memory_space=pltpu.VMEM)
    unit = pltpu.VMEM((plan.S, plan.R, plan.C, GD), jnp.bfloat16)
    return pl.pallas_call(
        functools.partial(mixer, plan),
        out_shape=[jax.ShapeDtypeStruct(value.shape, value.dtype)] * 2,
        in_specs=[anywhere] * 3 + [vmem] * 2,
        out_specs=[anywhere] * 2,
        scratch_shapes=[
            pltpu.VMEM(value.shape, value.dtype),
            pltpu.VMEM(value.shape, value.dtype),
            pltpu.VMEM((plan.S, plan.X, plan.PR * plan.T, plan.PW), jnp.bfloat16),
            unit, unit,
            pltpu.VMEM((plan.S, plan.R, plan.C), jnp.float32),
            dma, dma((plan.NI,)),
            dma, dma((plan.SH,)), dma, dma, dma, dma((plan.S,)), dma,
            dma((plan.SH, hop)), dma((plan.SH, hop)), dma, dma((plan.SH,)), dma, dma,
        ],
        compiler_params=pltpu.CompilerParams(
            collective_id=0, has_side_effects=True, vmem_limit_bytes=40 * 1024 * 1024
        ),
    )(w, bias, value, gain, shift)[0]


def body(sp, dp, gate_input, value_input, norm_gain, norm_bias, mix_weight, mix_bias):
    length, width = value_input.shape[1:]
    rows, blk = mix_weight.shape[1:]
    plan = Plan(sp, dp, length, width, rows, blk)
    bias = mix_bias[0].astype(jnp.float32).reshape(plan.R, plan.C)
    gain, shift = norm_gain.astype(jnp.float32)[None], norm_bias.astype(jnp.float32)[None]
    mixed = mix(plan, value_input[0], gain, shift, mix_weight[0], bias)
    gated = jax.nn.gelu(gate_input.astype(jnp.float32)) * mixed[None].astype(jnp.float32)
    return gated.astype(jnp.bfloat16)


def solution(mesh):
    placed = (
        P(("grp", "dp"), "sp", None),
        P(("grp", "dp"), "sp", None),
        P(),
        P(),
        P("sp", "dp", None),
        P("sp", None),
    )
    return jax.shard_map(
        functools.partial(body, mesh.shape["sp"], mesh.shape["dp"]),
        mesh=mesh, in_specs=placed, out_specs=P(("grp", "dp"), "sp", None), check_vma=False,
    )
```

```python
import functools

import jax
import jax.numpy as jnp
from jax import lax
from jax.experimental import pallas as pl
from jax.experimental.pallas import tpu as pltpu
from jax.sharding import PartitionSpec as P

GD = 128
BLK = 1024
MESH = pl.DeviceIdType.MESH


def div(a, n):
    if isinstance(a, int):
        return a // n
    return lax.shift_right_logical(a, n.bit_length() - 1) if n & (n - 1) == 0 else lax.div(a, n)


def mod(a, n):
    if isinstance(a, int):
        return a % n
    return lax.bitwise_and(a, n - 1) if n & (n - 1) == 0 else lax.rem(a, n)


class Plan:
    def __init__(self, sp, dp, length, width, rows, blk):
        self.sp, self.dp = sp, dp
        self.X = dp // 2
        self.C = rows * 2
        self.R = blk // self.C
        self.NI = length // self.C
        self.NB = sp * length // blk
        self.G = width // GD
        self.S = self.NB * self.G // sp
        self.SH = self.S // 2
        self.T = self.C // self.X
        self.PR = self.R // 2
        self.PW = self.C * (self.R + 1)
        self.HALF = self.X // 2
        far = 0
        for z in range(sp):
            for i in range(self.NI):
                for u in range(self.G):
                    far = max(far, abs((self.G * ((self.NI * z + i) // self.R) + u) // self.S - z))
        self.far = far

    def turn(self, b):
        return mod(self.G // 2 + self.G - div(self.G * b + self.G // 2, self.S), self.G)

    def group(self, p):
        b = div(p, self.G)
        return b, mod(p + self.G - self.turn(b), self.G)

    def item(self, b, g):
        return self.G * b + mod(g + self.turn(b), self.G)


def loop(n, body):
    def step(k, carry):
        body(k)
        return carry

    lax.fori_loop(0, n, step, 0)


def mixer(plan, w, value, scales, out, normed, vbuf, nbuf, bias, wbuf, xin, y, bbuf, vs, ns, w1s, w1r, bs, br, xs, xr, rs, rr, rl, ps, pr, ys, yr):
    X, C, R, NI, NB, G, S, SH, T, PR = (
        plan.X, plan.C, plan.R, plan.NI, plan.NB, plan.G, plan.S, plan.SH, plan.T, plan.PR,
    )
    z = lax.axis_index("sp")
    d = lax.axis_index("dp")
    x, c = div(d, 2), mod(d, 2)
    right = {"sp": z, "dp": 2 * mod(x + 1, X) + c}
    left = {"sp": z, "dp": 2 * mod(x + X - 1, X) + c}
    partner = {"sp": z, "dp": 2 * x + 1 - c}

    def remote(src, dst, send, recv, to):
        return pltpu.make_async_remote_copy(
            src_ref=src, dst_ref=dst, send_sem=send, recv_sem=recv, device_id=to, device_id_type=MESH
        )

    def put(src, dst, send, recv, sp, dp):
        here = jnp.logical_and(sp == z, dp == d)

        @pl.when(here)
        def _():
            pltpu.make_async_copy(src, dst, recv).start()

        @pl.when(jnp.logical_not(here))
        def _():
            remote(src, dst, send, recv, {"sp": sp, "dp": dp}).start()

    def arrived(ref, sem):
        pltpu.make_async_copy(ref, ref, sem).wait()

    def rows(k):
        return pl.ds(pl.multiple_of(k * C, C), C)

    load = pltpu.make_async_copy(value, vbuf, vs)
    load.start()
    for r in range(R):
        bias[r : r + 1, :] = scales[:, C * r : C * (r + 1)]

    bar = pltpu.get_barrier_semaphore()

    def greet(sp, dp):
        apart = jnp.logical_or(sp != z, dp != d)

        @pl.when(apart)
        def _():
            pl.semaphore_signal(bar, inc=1, device_id={"sp": sp, "dp": dp}, device_id_type=MESH)

        return apart.astype(jnp.int32)

    def greet_sources(jj, met):
        _, g = plan.group(S * z + SH * c + jj)
        return lax.fori_loop(0, X, lambda k, n: n + greet(g, 2 * k + div(x, plan.HALF)), met)

    met = lax.fori_loop(0, SH, greet_sources, jnp.int32(0))
    met = lax.fori_loop(0, S, lambda j, n: n + greet(plan.group(S * z + j)[1], d), met)
    for far in range(1, plan.far + 1):
        greet(mod(z + far, plan.sp), d)
        greet(mod(z + plan.sp - far, plan.sp), d)
    for to in (right, left, partner):
        pl.semaphore_signal(bar, inc=1, device_id=to, device_id_type=MESH)
    with jax.named_scope("barrier"):
        pl.semaphore_wait(bar, met + 2 * plan.far + 3)

    def first_leg(jj, k):
        ncol = C * (k + 1)
        row = min(k, R - 1 - k) * T
        col = 0 if k < R // 2 else C * (R - k)

        def one(b):
            p = plan.item(b, z)
            j, own = mod(p, S), div(p, S)

            @pl.when(mod(j, SH) == jj)
            def _():
                def strip(q):
                    xp = plan.HALF * c + q
                    put(
                        w.at[pl.ds(pl.multiple_of(q * T, T), T), pl.ds(0, ncol)],
                        wbuf.at[j, xp, pl.ds(row, T), pl.ds(col, ncol)],
                        w1s, w1r.at[jj], own, 2 * xp + div(j, SH),
                    )

                loop(plan.HALF, strip)

        loop(NB, one)

    def first_leg_gone():
        def kept(b, n):
            p = plan.item(b, z)
            return n + jnp.logical_and(div(p, S) == z, div(mod(p, S), SH) == c).astype(jnp.int32)

        own = lax.fori_loop(0, NB, kept, jnp.int32(0)) * (div(x, plan.HALF) == c).astype(jnp.int32)
        for k in range(X):
            @pl.when(x == k)
            def _(k=k):
                part = w.at[pl.ds(0, T), pl.ds(0, C * (k + 1))]
                loop(NB * plan.HALF - own, lambda _: arrived(part, w1s))

        def one(b):
            @pl.when(div(plan.item(b, z), S) != z)
            def _():
                arrived(bias, bs)

        loop(NB, one)

    def send_first_leg(jj):
        with jax.named_scope(f"leg1_{jj}"):
            for k in range(X):
                pl.when(x == k)(functools.partial(first_leg, jj, k))

    send_first_leg(0)

    def send_bias(b):
        p = plan.item(b, z)
        put(bias, bbuf.at[mod(p, S)], bs, br, div(p, S), d)

    loop(NB, send_bias)

    step_rows = min(16, C)

    def normalize(k):
        at = pl.ds(pl.multiple_of(k * step_rows, step_rows), step_rows)
        act = jax.nn.gelu(vbuf[at, :].astype(jnp.float32))
        mean = jnp.mean(act, axis=-1, keepdims=True)
        act = act - mean
        var = jnp.mean(jnp.square(act), axis=-1, keepdims=True)
        nbuf[at, :] = (act * lax.rsqrt(var + 1e-06) * scales[:, R * C : R * C + G * GD] + scales[:, R * C + G * GD :]).astype(nbuf.dtype)

    with jax.named_scope("normalize"):
        load.wait()
        for i in range(NI):
            loop(C // step_rows, lambda k, i=i: normalize(i * (C // step_rows) + k))
            pltpu.make_async_copy(nbuf.at[rows(i)], normed.at[rows(i)], ns.at[i]).start()
        for i in range(NI):
            arrived(nbuf.at[rows(i)], ns.at[i])

    per = -(-G // SH)

    def send_units(jj, n):
        def unit(k, n):
            i, t = div(k, per), mod(k, per)
            ch = NI * z + i
            b, r = div(ch, R), mod(ch, R)
            u = mod(jj + G * SH * NB - G * b, SH) + SH * t
            p = G * b + u

            @pl.when(u < G)
            def _():
                g = plan.group(p)[1]
                src = normed.at[rows(i), pl.ds(pl.multiple_of(g * GD, GD), GD)]
                put(src, xin.at[mod(p, S), r], xs, xr.at[mod(p, S)], div(p, S), d)

            return n + jnp.logical_and(u < G, div(p, S) != z).astype(jnp.int32)

        with jax.named_scope(f"units{jj}"):
            return lax.fori_loop(0, NI * per, unit, n)

    hops = plan.HALF

    def pass_on(jj, blk, send, recv, to):
        remote(wbuf.at[SH * c + jj, blk], wbuf.at[SH * c + jj, blk], send, recv, to).start()

    def ring(jj, s):
        more = mod(jj + c, 2) == 0
        if s == 0:
            arrived(wbuf.at[SH * c + jj, x], w1r.at[jj])
            blk = x
            if X - hops - 1 >= 1:
                pass_on(jj, blk, rs, rr.at[jj, 0], right)
                pass_on(jj, blk, rs, rl.at[jj, 0], left)
            else:
                @pl.when(more)
                def _():
                    pass_on(jj, blk, rs, rr.at[jj, 0], right)

                @pl.when(jnp.logical_not(more))
                def _():
                    pass_on(jj, blk, rs, rl.at[jj, 0], left)
            pass_on(jj, blk, ps, pr.at[jj], partner)
            return
        for sems, to, blk, longer in (
            (rr, right, mod(x + X - s, X), more),
            (rl, left, mod(x + s, X), jnp.logical_not(more)),
        ):
            def step(forward, sems=sems, to=to, blk=blk):
                arrived(wbuf.at[SH * c + jj, blk], sems.at[jj, s - 1])
                if forward is True:
                    pass_on(jj, blk, rs, sems.at[jj, s], to)
                elif forward is not False:
                    @pl.when(forward)
                    def _():
                        pass_on(jj, blk, rs, sems.at[jj, s], to)
                pass_on(jj, blk, ps, pr.at[jj], partner)

            if s < hops - 1:
                step(True)
            elif s < hops:
                step(longer)
            else:
                pl.when(longer)(functools.partial(step, False))

    def compute(jj, other):
        co = jnp.where(other == 1, 1 - c, c)
        j = SH * co + jj
        b, g = plan.group(S * z + j)
        arrived(xin.at[j], xr.at[j])
        bcol = jnp.transpose(bbuf[j])
        keep = lax.broadcasted_iota(jnp.int32, (C, C), 1) <= lax.broadcasted_iota(jnp.int32, (C, C), 0)
        for r in range(R):
            row = min(r, R - 1 - r) * T
            col = 0 if r < R // 2 else C * (R - r)
            diag = wbuf[j, :, row : row + T, col + C * r : col + C * (r + 1)].reshape(C, C)
            diag = jnp.where(keep, diag, jnp.zeros_like(diag))
            acc = jnp.dot(diag, xin[j, r], preferred_element_type=jnp.float32)
            if r:
                before = wbuf[j, :, row : row + T, col : col + C * r].reshape(C, C * r)
                acc += jnp.dot(before, xin[j, :r].reshape(C * r, GD), preferred_element_type=jnp.float32)
            y[j, r] = (acc + bcol[:, r : r + 1]).astype(y.dtype)

        def give(r):
            ch = R * b + r
            sp, i = div(ch, NI), mod(ch, NI)
            dst = out.at[pl.ds(pl.multiple_of(i * C, C), C), pl.ds(pl.multiple_of(g * GD, GD), GD)]
            put(y.at[j, r], dst, ys, yr, sp, d)

        loop(R, give)

    last = hops

    def finish(jj):
        with jax.named_scope(f"partner{jj}"):
            arrived(wbuf.at[SH * (1 - c) + jj], pr.at[jj])
            if jj == 0:
                arrived(bbuf, br)
        with jax.named_scope(f"compute{jj}"):
            loop(2, functools.partial(compute, jj))

    order = sorted((s + 2 * jj, jj, s) for jj in range(SH) for s in range(last + 1))
    sent = jnp.int32(0)
    pending = None
    for _, jj, s in order:
        with jax.named_scope(f"ring{jj}_{s}"):
            ring(jj, s)
        if s == 0 and jj + 1 < SH:
            send_first_leg(jj + 1)
        if s == 1 or last == 0:
            sent = send_units(jj, sent)
        if pending is not None:
            finish(pending)
            pending = None
        if s == last:
            pending = jj
        if (jj, s) == (SH - 1, 1):
            with jax.named_scope("leg1_gone"):
                first_leg_gone()
    finish(pending)
    with jax.named_scope("sends_gone"):
        loop(sent, lambda _: arrived(xin.at[0, 0], xs))
        loop(SH * (X - 1), lambda k: arrived(wbuf.at[0, 0], rs))
        loop(SH * X, lambda k: arrived(wbuf.at[0, 0], ps))
    with jax.named_scope("out_wait"):
        arrived(out, yr)
    with jax.named_scope("drain"):
        loop(sent, lambda _: arrived(y.at[0, 0], ys))


def mix(plan, value, scales, w):
    hop = max(plan.HALF, 1)
    dma = pltpu.SemaphoreType.DMA
    anywhere, vmem = pl.BlockSpec(memory_space=pl.ANY), pl.BlockSpec(memory_space=pltpu.VMEM)
    unit = pltpu.VMEM((plan.S, plan.R, plan.C, GD), jnp.bfloat16)
    return pl.pallas_call(
        functools.partial(mixer, plan),
        out_shape=[jax.ShapeDtypeStruct(value.shape, value.dtype)] * 2,
        in_specs=[anywhere, anywhere, vmem],
        out_specs=[anywhere] * 2,
        scratch_shapes=[
            pltpu.VMEM(value.shape, value.dtype),
            pltpu.VMEM(value.shape, value.dtype),
            pltpu.VMEM((plan.R, plan.C), jnp.float32),
            pltpu.VMEM((plan.S, plan.X, plan.PR * plan.T, plan.PW), jnp.bfloat16),
            unit, unit,
            pltpu.VMEM((plan.S, plan.R, plan.C), jnp.float32),
            dma, dma((plan.NI,)),
            dma, dma((plan.SH,)), dma, dma, dma, dma((plan.S,)), dma,
            dma((plan.SH, hop)), dma((plan.SH, hop)), dma, dma((plan.SH,)), dma, dma,
        ],
        compiler_params=pltpu.CompilerParams(
            collective_id=0, has_side_effects=True, vmem_limit_bytes=60 * 1024 * 1024
        ),
    )(w, value, scales)[0]


def body(sp, dp, gate_input, value_input, norm_gain, norm_bias, mix_weight, mix_bias):
    length, width = value_input.shape[1:]
    rows, blk = mix_weight.shape[1:]
    plan = Plan(sp, dp, length, width, rows, blk)
    scales = jnp.concatenate([mix_bias[0], norm_gain, norm_bias]).astype(jnp.float32)[None]
    mixed = mix(plan, value_input[0], scales, mix_weight[0])
    gated = jax.nn.gelu(gate_input.astype(jnp.float32)) * mixed[None].astype(jnp.float32)
    return gated.astype(jnp.bfloat16)


def solution(mesh):
    placed = (
        P(("grp", "dp"), "sp", None),
        P(("grp", "dp"), "sp", None),
        P(),
        P(),
        P("sp", "dp", None),
        P("sp", None),
    )
    return jax.shard_map(
        functools.partial(body, mesh.shape["sp"], mesh.shape["dp"]),
        mesh=mesh, in_specs=placed, out_specs=P(("grp", "dp"), "sp", None), check_vma=False,
    )
```

```python
import functools

import jax
import jax.numpy as jnp
from jax import lax
from jax.experimental import pallas as pl
from jax.experimental.pallas import tpu as pltpu
from jax.sharding import PartitionSpec as P

GD = 128
BLK = 1024
MESH = pl.DeviceIdType.MESH


def div(a, n):
    if isinstance(a, int):
        return a // n
    return lax.shift_right_logical(a, n.bit_length() - 1) if n & (n - 1) == 0 else lax.div(a, n)


def mod(a, n):
    if isinstance(a, int):
        return a % n
    return lax.bitwise_and(a, n - 1) if n & (n - 1) == 0 else lax.rem(a, n)


class Plan:
    def __init__(self, sp, dp, length, width, rows, blk):
        self.sp, self.dp = sp, dp
        self.X = dp // 2
        self.C = rows * 2
        self.R = blk // self.C
        self.NI = length // self.C
        self.NB = sp * length // blk
        self.G = width // GD
        self.S = self.NB * self.G // sp
        self.SH = self.S // 2
        self.T = self.C // self.X
        self.PR = self.R // 2
        self.PW = self.C * (self.R + 1)
        self.HALF = self.X // 2
        assert self.G % 5 and self.G & (self.G - 1) == 0
        far = 0
        for z in range(sp):
            for i in range(self.NI):
                for u in range(self.G):
                    far = max(far, abs((self.G * ((self.NI * z + i) // self.R) + u) // self.S - z))
        self.far = far

    def group(self, p):
        return div(p, self.G), mod(mod(p, self.G) * 5, self.G)

    def item(self, b, g):
        return self.G * b + mod(g * pow(5, -1, self.G), self.G)


def loop(n, body):
    def step(k, carry):
        body(k)
        return carry

    lax.fori_loop(0, n, step, 0)


def mixer(plan, w, value, scales, out, normed, vbuf, nbuf, bias, wbuf, sblk, xin, y, bbuf, vs, ns, l0s, l0r, rdn, rdw, w1s, w1r, bs, br, xs, xr, rs, rr, rl, ps, pr, ys, yr):
    X, C, R, NI, NB, G, S, SH, T, PR = (
        plan.X, plan.C, plan.R, plan.NI, plan.NB, plan.G, plan.S, plan.SH, plan.T, plan.PR,
    )
    z = lax.axis_index("sp")
    d = lax.axis_index("dp")
    x, c = div(d, 2), mod(d, 2)
    right = {"sp": z, "dp": 2 * mod(x + 1, X) + c}
    left = {"sp": z, "dp": 2 * mod(x + X - 1, X) + c}
    partner = {"sp": z, "dp": 2 * x + 1 - c}

    def remote(src, dst, send, recv, to):
        return pltpu.make_async_remote_copy(
            src_ref=src, dst_ref=dst, send_sem=send, recv_sem=recv, device_id=to, device_id_type=MESH
        )

    def put(src, dst, send, recv, sp, dp):
        here = jnp.logical_and(sp == z, dp == d)

        @pl.when(here)
        def _():
            pltpu.make_async_copy(src, dst, recv).start()

        @pl.when(jnp.logical_not(here))
        def _():
            remote(src, dst, send, recv, {"sp": sp, "dp": dp}).start()

    def arrived(ref, sem):
        pltpu.make_async_copy(ref, ref, sem).wait()

    def rows(k):
        return pl.ds(pl.multiple_of(k * C, C), C)

    load = pltpu.make_async_copy(value, vbuf, vs)
    load.start()
    for r in range(R):
        bias[r : r + 1, :] = scales[:, C * r : C * (r + 1)]

    bar = pltpu.get_barrier_semaphore()

    def greet(sp, dp):
        pl.semaphore_signal(bar, inc=1, device_id={"sp": sp, "dp": dp}, device_id_type=MESH)

    def owner(b):
        return div(plan.item(b, z), S)

    def source(j):
        return plan.group(S * z + j)

    def greet_plane(k, n):
        dp = 2 * k + div(x, plan.HALF)
        pl.when(dp != d)(lambda: greet(z, dp))
        return n + (dp != d).astype(jnp.int32)

    def greet_owner(b, n):
        up = owner(b)
        pl.when(up > z)(lambda: greet(up, d))
        return n + (up < z).astype(jnp.int32)

    def greet_source(j, n):
        up = source(j)[1]
        pl.when(up > z)(lambda: greet(up, d))
        return n + (up < z).astype(jnp.int32)

    for to in (right, left, partner):
        pl.semaphore_signal(bar, inc=1, device_id=to, device_id_type=MESH)
    met = lax.fori_loop(0, X, greet_plane, jnp.int32(3))
    for far in range(1, plan.far + 1):
        pl.when(z + far < plan.sp)(functools.partial(greet, z + far, d))
        met += (z >= far).astype(jnp.int32)
    met = lax.fori_loop(0, NB, greet_owner, met)
    met = lax.fori_loop(0, S, greet_source, met)
    with jax.named_scope("barrier"):
        pl.semaphore_wait(bar, met)

    def plane_leg(k):
        ncol = C * (k + 1)
        row = min(k, R - 1 - k) * T
        col = 0 if k < R // 2 else C * (R - k)

        def strip(n):
            q, core = div(n, 2), mod(n, 2)
            put(
                w.at[pl.ds(pl.multiple_of(q * T, T), T), pl.ds(0, ncol)],
                sblk.at[pl.ds(row, T), pl.ds(col, ncol)],
                l0s, l0r, z, 2 * (plan.HALF * c + q) + core,
            )

        loop(2 * plan.HALF, strip)

    with jax.named_scope("plane_leg"):
        for k in range(X):
            pl.when(x == k)(functools.partial(plane_leg, k))

    def ready(j):
        b, g = source(j)

        @pl.when(g < z)
        def _():
            pl.semaphore_signal(rdw.at[b], inc=1, device_id={"sp": g, "dp": d}, device_id_type=MESH)

    loop(S, ready)
    for far in range(1, plan.far + 1):
        @pl.when(z >= far)
        def _(far=far):
            pl.semaphore_signal(rdn.at[far - 1], inc=1, device_id={"sp": z - far, "dp": d}, device_id_type=MESH)

    def give_weights(b):
        p = plan.item(b, z)
        j, own = mod(p, S), div(p, S)
        mine = div(j, SH) == c

        @pl.when(own == z)
        def _():
            pltpu.make_async_copy(bias, bbuf.at[j], br).start()

            @pl.when(mine)
            def _():
                wbuf[j, x] = sblk[...]

        @pl.when(own != z)
        def _():
            to = {"sp": own, "dp": d}
            remote(bias, bbuf.at[j], bs, br, to).start()

            @pl.when(mine)
            def _():
                remote(sblk, wbuf.at[j, x], w1s, w1r.at[mod(j, SH)], to).start()

    def give_down(b):
        pl.when(owner(b) <= z)(lambda: give_weights(b))

    def give_up(b):
        with jax.named_scope(f"give_up{b}"):
            @pl.when(owner(b) > z)
            def _():
                pl.semaphore_wait(rdw.at[b], 1)
                give_weights(b)

    def weights_gone():
        for k in range(X):
            @pl.when(x == k)
            def _(k=k):
                part = w.at[pl.ds(0, T), pl.ds(0, C * (k + 1))]
                own = (div(x, plan.HALF) == c).astype(jnp.int32)
                loop(2 * plan.HALF - own, lambda _: arrived(part, l0s))

        def one(b):
            @pl.when(owner(b) != z)
            def _():
                arrived(bias, bs)

                @pl.when(div(mod(plan.item(b, z), S), SH) == c)
                def _():
                    arrived(sblk, w1s)

        loop(NB, one)

    step_rows = min(16, C)

    def normalize(k):
        at = pl.ds(pl.multiple_of(k * step_rows, step_rows), step_rows)
        act = jax.nn.gelu(vbuf[at, :].astype(jnp.float32))
        mean = jnp.mean(act, axis=-1, keepdims=True)
        act = act - mean
        var = jnp.mean(jnp.square(act), axis=-1, keepdims=True)
        nbuf[at, :] = (act * lax.rsqrt(var + 1e-06) * scales[:, R * C : R * C + G * GD] + scales[:, R * C + G * GD :]).astype(nbuf.dtype)

    with jax.named_scope("normalize"):
        load.wait()
        for i in range(NI):
            def two(k, i=i):
                normalize(i * (C // step_rows) + 2 * k)
                normalize(i * (C // step_rows) + 2 * k + 1)

            loop(C // step_rows // 2, two)
            pltpu.make_async_copy(nbuf.at[rows(i)], normed.at[rows(i)], ns.at[i]).start()
        for i in range(NI):
            arrived(nbuf.at[rows(i)], ns.at[i])

    with jax.named_scope("plane_wait"):
        arrived(sblk, l0r)
        loop(NB, give_down)

    def send_units(wanted):
        def unit(k, n):
            i, g = div(k, G), mod(k, G)
            ch = NI * z + i
            b, r = div(ch, R), mod(ch, R)
            p = plan.item(b, g)
            own = div(p, S)

            @pl.when(wanted(own))
            def _():
                src = normed.at[rows(i), pl.ds(pl.multiple_of(g * GD, GD), GD)]
                put(src, xin.at[mod(p, S), r], xs, xr.at[mod(p, S)], own, d)

            return n + (own != z).astype(jnp.int32)

        return lax.fori_loop(0, NI * G, unit, jnp.int32(0))

    with jax.named_scope("units_down"):
        sent = send_units(lambda own: own <= z)
    for far in range(1, plan.far + 1):
        with jax.named_scope(f"units_up{far}"):
            @pl.when(z + far < plan.sp)
            def _(far=far):
                pl.semaphore_wait(rdn.at[far - 1], 1)
                send_units(lambda own: own == z + far)

    hops = plan.HALF

    def ranked(core):
        keys = [jnp.maximum(source(SH * core + k)[1], z) * SH + k for k in range(SH)]
        ranks = [sum((a < b).astype(jnp.int32) for a in keys) for b in keys]
        return [SH * core + sum(k * (ranks[k] == n).astype(jnp.int32) for k in range(SH)) for n in range(SH)]

    mine, theirs = ranked(c), ranked(1 - c)

    def pass_on(jj, blk, send, recv, to):
        remote(wbuf.at[mine[jj], blk], wbuf.at[mine[jj], blk], send, recv, to).start()

    def ring(jj, s):
        more = mod(jj + c, 2) == 0
        if s == 0:
            @pl.when(source(mine[jj])[1] != z)
            def _():
                arrived(wbuf.at[mine[jj], x], w1r.at[mod(mine[jj], SH)])

            blk = x
            if X - hops - 1 >= 1:
                pass_on(jj, blk, rs, rr.at[jj, 0], right)
                pass_on(jj, blk, rs, rl.at[jj, 0], left)
            else:
                @pl.when(more)
                def _():
                    pass_on(jj, blk, rs, rr.at[jj, 0], right)

                @pl.when(jnp.logical_not(more))
                def _():
                    pass_on(jj, blk, rs, rl.at[jj, 0], left)
            pass_on(jj, blk, ps, pr.at[jj], partner)
            return
        for sems, to, blk, longer in (
            (rr, right, mod(x + X - s, X), more),
            (rl, left, mod(x + s, X), jnp.logical_not(more)),
        ):
            def step(forward, sems=sems, to=to, blk=blk):
                arrived(wbuf.at[mine[jj], blk], sems.at[jj, s - 1])
                if forward is True:
                    pass_on(jj, blk, rs, sems.at[jj, s], to)
                elif forward is not False:
                    @pl.when(forward)
                    def _():
                        pass_on(jj, blk, rs, sems.at[jj, s], to)
                pass_on(jj, blk, ps, pr.at[jj], partner)

            if s < hops - 1:
                step(True)
            elif s < hops:
                step(longer)
            else:
                pl.when(longer)(functools.partial(step, False))

    def compute(jj, other):
        j = jnp.where(other == 1, theirs[jj], mine[jj])
        b, g = plan.group(S * z + j)
        arrived(xin.at[j], xr.at[j])
        bcol = jnp.transpose(bbuf[j])
        keep = lax.broadcasted_iota(jnp.int32, (C, C), 1) <= lax.broadcasted_iota(jnp.int32, (C, C), 0)
        for r in range(R):
            row = min(r, R - 1 - r) * T
            col = 0 if r < R // 2 else C * (R - r)
            diag = wbuf[j, :, row : row + T, col + C * r : col + C * (r + 1)].reshape(C, C)
            diag = jnp.where(keep, diag, jnp.zeros_like(diag))
            acc = jnp.dot(diag, xin[j, r], preferred_element_type=jnp.float32)
            if r:
                before = wbuf[j, :, row : row + T, col : col + C * r].reshape(C, C * r)
                acc += jnp.dot(before, xin[j, :r].reshape(C * r, GD), preferred_element_type=jnp.float32)
            y[j, r] = (acc + bcol[:, r : r + 1]).astype(y.dtype)

        def give(r):
            ch = R * b + r
            sp, i = div(ch, NI), mod(ch, NI)
            dst = out.at[pl.ds(pl.multiple_of(i * C, C), C), pl.ds(pl.multiple_of(g * GD, GD), GD)]
            put(y.at[j, r], dst, ys, yr, sp, d)

        loop(R, give)

    last = hops

    def finish(jj):
        with jax.named_scope(f"partner{jj}"):
            arrived(wbuf.at[theirs[jj]], pr.at[jj])
            if jj == 0:
                arrived(bbuf, br)
        with jax.named_scope(f"compute{jj}"):
            loop(2, functools.partial(compute, jj))

    order = sorted((s + 2 * jj, jj, s) for jj in range(SH) for s in range(last + 1))
    at = {}
    for b in range(NB):
        at.setdefault(min(max(0, 2 * (b - NB // 2) + 2) if b >= NB // 2 else 0, len(order) - 1), []).append(b)
    pending = None
    for n, (_, jj, s) in enumerate(order):
        for b in at.get(n, []):
            give_up(b)
        with jax.named_scope(f"ring{jj}_{s}"):
            ring(jj, s)
        if pending is not None:
            finish(pending)
            pending = None
        if s == last:
            pending = jj
        if n == len(order) - 3:
            with jax.named_scope("weights_gone"):
                weights_gone()
    finish(pending)
    with jax.named_scope("sends_gone"):
        loop(sent, lambda _: arrived(xin.at[0, 0], xs))
        loop(SH * (X - 1), lambda k: arrived(wbuf.at[0, 0], rs))
        loop(SH * X, lambda k: arrived(wbuf.at[0, 0], ps))
    with jax.named_scope("out_wait"):
        arrived(out, yr)
    with jax.named_scope("drain"):
        loop(sent, lambda _: arrived(y.at[0, 0], ys))


def mix(plan, value, scales, w):
    hop = max(plan.HALF, 1)
    dma = pltpu.SemaphoreType.DMA
    anywhere, vmem = pl.BlockSpec(memory_space=pl.ANY), pl.BlockSpec(memory_space=pltpu.VMEM)
    unit = pltpu.VMEM((plan.S, plan.R, plan.C, GD), jnp.bfloat16)
    return pl.pallas_call(
        functools.partial(mixer, plan),
        out_shape=[jax.ShapeDtypeStruct(value.shape, value.dtype)] * 2,
        in_specs=[anywhere, anywhere, vmem],
        out_specs=[anywhere] * 2,
        scratch_shapes=[
            pltpu.VMEM(value.shape, value.dtype),
            pltpu.VMEM(value.shape, value.dtype),
            pltpu.VMEM((plan.R, plan.C), jnp.float32),
            pltpu.VMEM((plan.S, plan.X, plan.PR * plan.T, plan.PW), jnp.bfloat16),
            pltpu.VMEM((plan.PR * plan.T, plan.PW), jnp.bfloat16),
            unit, unit,
            pltpu.VMEM((plan.S, plan.R, plan.C), jnp.float32),
            dma, dma((plan.NI,)), dma, dma,
            pltpu.SemaphoreType.REGULAR((plan.far,)), pltpu.SemaphoreType.REGULAR((plan.NB,)),
            dma, dma((plan.SH,)), dma, dma, dma, dma((plan.S,)), dma,
            dma((plan.SH, hop)), dma((plan.SH, hop)), dma, dma((plan.SH,)), dma, dma,
        ],
        compiler_params=pltpu.CompilerParams(
            collective_id=0, has_side_effects=True, vmem_limit_bytes=60 * 1024 * 1024
        ),
    )(w, value, scales)[0]


def body(sp, dp, gate_input, value_input, norm_gain, norm_bias, mix_weight, mix_bias):
    length, width = value_input.shape[1:]
    rows, blk = mix_weight.shape[1:]
    plan = Plan(sp, dp, length, width, rows, blk)
    scales = jnp.concatenate([mix_bias[0], norm_gain, norm_bias]).astype(jnp.float32)[None]
    mixed = mix(plan, value_input[0], scales, mix_weight[0])
    gated = jax.nn.gelu(gate_input.astype(jnp.float32)) * mixed[None].astype(jnp.float32)
    return gated.astype(jnp.bfloat16)


def solution(mesh):
    placed = (
        P(("grp", "dp"), "sp", None),
        P(("grp", "dp"), "sp", None),
        P(),
        P(),
        P("sp", "dp", None),
        P("sp", None),
    )
    return jax.shard_map(
        functools.partial(body, mesh.shape["sp"], mesh.shape["dp"]),
        mesh=mesh, in_specs=placed, out_specs=P(("grp", "dp"), "sp", None), check_vma=False,
    )
```

```python
import functools

import jax
import jax.numpy as jnp
from jax import lax
from jax.experimental import pallas as pl
from jax.experimental.pallas import tpu as pltpu
from jax.sharding import PartitionSpec as P

GD = 128
BLK = 1024
MESH = pl.DeviceIdType.MESH


def div(a, n):
    if isinstance(a, int):
        return a // n
    if n & (n - 1) == 0:
        return lax.shift_right_logical(a, n.bit_length() - 1)
    return lax.shift_right_logical(a * (65536 // n + 1), 16)


def mod(a, n):
    if isinstance(a, int):
        return a % n
    return lax.bitwise_and(a, n - 1) if n & (n - 1) == 0 else a - n * div(a, n)


class Plan:
    def __init__(self, sp, dp, length, width, rows, blk):
        self.sp, self.dp = sp, dp
        self.X = dp // 2
        self.C = rows * 2
        self.R = blk // self.C
        self.NI = length // self.C
        self.NB = sp * length // blk
        self.G = width // GD
        self.S = self.NB * self.G // sp
        self.SH = self.S // 2
        self.T = self.C // self.X
        self.PR = self.R // 2
        self.PW = self.C * (self.R + 1)
        self.HALF = self.X // 2
        assert self.G % 5 and self.G & (self.G - 1) == 0
        far = 0
        for z in range(sp):
            for i in range(self.NI):
                for u in range(self.G):
                    far = max(far, abs((self.G * ((self.NI * z + i) // self.R) + u) // self.S - z))
        self.far = far

    def group(self, p):
        return div(p, self.G), mod(mod(p, self.G) * 5, self.G)

    def item(self, b, g):
        return self.G * b + mod(g * pow(5, -1, self.G), self.G)


def loop(n, body):
    def step(k, carry):
        body(k)
        return carry

    lax.fori_loop(0, n, step, 0)


def mixer(plan, w, value, mix_bias, norm_gain, norm_bias, out, normed, vbuf, nbuf, bias, wbuf, sblk, xin, y, bbuf, vs, ns, l0s, l0r, rdn, rdw, w1s, w1r, bs, br, xs, xr, rs, rr, rl, ps, pr, ys, yr):
    X, C, R, NI, NB, G, S, SH, T, PR = (
        plan.X, plan.C, plan.R, plan.NI, plan.NB, plan.G, plan.S, plan.SH, plan.T, plan.PR,
    )
    z = lax.axis_index("sp")
    d = lax.axis_index("dp")
    x, c = div(d, 2), mod(d, 2)
    right = {"sp": z, "dp": 2 * mod(x + 1, X) + c}
    left = {"sp": z, "dp": 2 * mod(x + X - 1, X) + c}
    partner = {"sp": z, "dp": 2 * x + 1 - c}

    def remote(src, dst, send, recv, to):
        return pltpu.make_async_remote_copy(
            src_ref=src, dst_ref=dst, send_sem=send, recv_sem=recv, device_id=to, device_id_type=MESH
        )

    def put(src, dst, send, recv, sp, dp):
        here = jnp.logical_and(sp == z, dp == d)

        @pl.when(here)
        def _():
            pltpu.make_async_copy(src, dst, recv).start()

        @pl.when(jnp.logical_not(here))
        def _():
            remote(src, dst, send, recv, {"sp": sp, "dp": dp}).start()

    def arrived(ref, sem):
        pltpu.make_async_copy(ref, ref, sem).wait()

    def rows(k):
        return pl.ds(pl.multiple_of(k * C, C), C)

    load = pltpu.make_async_copy(value, vbuf, vs)
    load.start()

    bar = pltpu.get_barrier_semaphore()

    def greet(sp, dp):
        pl.semaphore_signal(bar, inc=1, device_id={"sp": sp, "dp": dp}, device_id_type=MESH)

    def owner(b):
        return div(plan.item(b, z), S)

    def source(j):
        return plan.group(S * z + j)

    def greet_plane(k, n):
        dp = 2 * k + div(x, plan.HALF)
        pl.when(dp != d)(lambda: greet(z, dp))
        return n + (dp != d).astype(jnp.int32)

    def greet_owner(b, n):
        up = owner(b)
        pl.when(up > z)(lambda: greet(up, d))
        return n + (up < z).astype(jnp.int32)

    def greet_source(j, n):
        up = source(j)[1]
        pl.when(up > z)(lambda: greet(up, d))
        return n + (up < z).astype(jnp.int32)

    for to in (right, left, partner):
        pl.semaphore_signal(bar, inc=1, device_id=to, device_id_type=MESH)
    met = jnp.int32(3)
    for k in range(X):
        met = greet_plane(k, met)
    for far in range(1, plan.far + 1):
        pl.when(z + far < plan.sp)(functools.partial(greet, z + far, d))
        met += (z >= far).astype(jnp.int32)
    for b in range(NB):
        met = greet_owner(b, met)
    for j in range(S):
        met = greet_source(j, met)
    with jax.named_scope("barrier"):
        pl.semaphore_wait(bar, met)

    def plane_leg(k):
        ncol = C * (k + 1)
        row = min(k, R - 1 - k) * T
        col = 0 if k < R // 2 else C * (R - k)

        def strip(n):
            q, core = div(n, 2), mod(n, 2)
            put(
                w.at[pl.ds(pl.multiple_of(q * T, T), T), pl.ds(0, ncol)],
                sblk.at[pl.ds(row, T), pl.ds(col, ncol)],
                l0s, l0r, z, 2 * (plan.HALF * c + q) + core,
            )

        loop(2 * plan.HALF, strip)

    for r in range(R):
        bias[r : r + 1, :] = mix_bias[:, C * r : C * (r + 1)].astype(jnp.float32)

    with jax.named_scope("plane_leg"):
        for k in range(X):
            pl.when(x == k)(functools.partial(plane_leg, k))

    def ready(j):
        b, g = source(j)

        @pl.when(g < z)
        def _():
            pl.semaphore_signal(rdw.at[b], inc=1, device_id={"sp": g, "dp": d}, device_id_type=MESH)

    loop(S, ready)
    for far in range(1, plan.far + 1):
        @pl.when(z >= far)
        def _(far=far):
            pl.semaphore_signal(rdn.at[far - 1], inc=1, device_id={"sp": z - far, "dp": d}, device_id_type=MESH)

    def give_weights(b):
        p = plan.item(b, z)
        j, own = mod(p, S), div(p, S)
        mine = div(j, SH) == c

        @pl.when(own == z)
        def _():
            pltpu.make_async_copy(bias, bbuf.at[j], br).start()

            @pl.when(mine)
            def _():
                wbuf[j, x] = sblk[...]

        @pl.when(own != z)
        def _():
            to = {"sp": own, "dp": d}
            remote(bias, bbuf.at[j], bs, br, to).start()

            @pl.when(mine)
            def _():
                remote(sblk, wbuf.at[j, x], w1s, w1r.at[mod(j, SH)], to).start()

    def give_down(b):
        pl.when(owner(b) <= z)(lambda: give_weights(b))

    def give_up(b):
        with jax.named_scope(f"give_up{b}"):
            @pl.when(owner(b) > z)
            def _():
                pl.semaphore_wait(rdw.at[b], 1)
                give_weights(b)

    def weights_gone():
        for k in range(X):
            @pl.when(x == k)
            def _(k=k):
                part = w.at[pl.ds(0, T), pl.ds(0, C * (k + 1))]
                own = (div(x, plan.HALF) == c).astype(jnp.int32)
                loop(2 * plan.HALF - own, lambda _: arrived(part, l0s))

        def one(b):
            @pl.when(owner(b) != z)
            def _():
                arrived(bias, bs)

                @pl.when(div(mod(plan.item(b, z), S), SH) == c)
                def _():
                    arrived(sblk, w1s)

        loop(NB, one)

    with jax.named_scope("plane_wait"):
        arrived(sblk, l0r)
        loop(NB, give_down)
    for b in range(NB // 2):
        give_up(b)

    step_rows = min(16, C)

    def normalize(k):
        at = pl.ds(pl.multiple_of(k * step_rows, step_rows), step_rows)
        act = jax.nn.gelu(vbuf[at, :].astype(jnp.float32))
        mean = jnp.mean(act, axis=-1, keepdims=True)
        act = act - mean
        var = jnp.mean(jnp.square(act), axis=-1, keepdims=True)
        nbuf[at, :] = (act * lax.rsqrt(var + 1e-06) * gain + shift).astype(nbuf.dtype)

    gain = norm_gain[...].astype(jnp.float32).reshape(1, G * GD)
    shift = norm_bias[...].astype(jnp.float32).reshape(1, G * GD)
    with jax.named_scope("normalize"):
        load.wait()
        for i in range(NI):
            def two(k, i=i):
                normalize(i * (C // step_rows) + 2 * k)
                normalize(i * (C // step_rows) + 2 * k + 1)

            loop(C // step_rows // 2, two)
            pltpu.make_async_copy(nbuf.at[rows(i)], normed.at[rows(i)], ns.at[i]).start()
        for i in range(NI):
            arrived(nbuf.at[rows(i)], ns.at[i])

    def send_units(wanted):
        def unit(k, n):
            i, g = div(k, G), mod(k, G)
            ch = NI * z + i
            b, r = div(ch, R), mod(ch, R)
            p = plan.item(b, g)
            own = div(p, S)

            @pl.when(wanted(own))
            def _():
                src = normed.at[rows(i), pl.ds(pl.multiple_of(g * GD, GD), GD)]
                put(src, xin.at[mod(p, S), r], xs, xr.at[mod(p, S)], own, d)

            return n + (own != z).astype(jnp.int32)

        return lax.fori_loop(0, NI * G, unit, jnp.int32(0))

    with jax.named_scope("units_down"):
        sent = send_units(lambda own: own <= z)
    for far in range(1, plan.far + 1):
        with jax.named_scope(f"units_up{far}"):
            @pl.when(z + far < plan.sp)
            def _(far=far):
                pl.semaphore_wait(rdn.at[far - 1], 1)
                send_units(lambda own: own == z + far)

    hops = plan.HALF

    def ranked(core):
        groups = [source(SH * core + k)[1] for k in range(SH)]
        keys = [jnp.where(g >= z, g, 2 * z - g) * SH + k for k, g in enumerate(groups)]
        ranks = [sum((a < b).astype(jnp.int32) for a in keys) for b in keys]
        return [SH * core + sum(k * (ranks[k] == n).astype(jnp.int32) for k in range(SH)) for n in range(SH)]

    mine, theirs = ranked(c), ranked(1 - c)

    def pass_on(jj, blk, send, recv, to):
        remote(wbuf.at[mine[jj], blk], wbuf.at[mine[jj], blk], send, recv, to).start()

    def ring(jj, s):
        more = mod(jj + c, 2) == 0
        if s == 0:
            @pl.when(source(mine[jj])[1] != z)
            def _():
                arrived(wbuf.at[mine[jj], x], w1r.at[mod(mine[jj], SH)])

            blk = x
            if X - hops - 1 >= 1:
                pass_on(jj, blk, rs, rr.at[jj, 0], right)
                pass_on(jj, blk, rs, rl.at[jj, 0], left)
            else:
                @pl.when(more)
                def _():
                    pass_on(jj, blk, rs, rr.at[jj, 0], right)

                @pl.when(jnp.logical_not(more))
                def _():
                    pass_on(jj, blk, rs, rl.at[jj, 0], left)
            pass_on(jj, blk, ps, pr.at[jj], partner)
            return
        for sems, to, blk, longer in (
            (rr, right, mod(x + X - s, X), more),
            (rl, left, mod(x + s, X), jnp.logical_not(more)),
        ):
            def step(forward, sems=sems, to=to, blk=blk):
                arrived(wbuf.at[mine[jj], blk], sems.at[jj, s - 1])
                if forward is True:
                    pass_on(jj, blk, rs, sems.at[jj, s], to)
                elif forward is not False:
                    @pl.when(forward)
                    def _():
                        pass_on(jj, blk, rs, sems.at[jj, s], to)
                pass_on(jj, blk, ps, pr.at[jj], partner)

            if s < hops - 1:
                step(True)
            elif s < hops:
                step(longer)
            else:
                pl.when(longer)(functools.partial(step, False))

    def compute(jj, other):
        j = jnp.where(other == 1, theirs[jj], mine[jj])
        b, g = plan.group(S * z + j)
        arrived(xin.at[j], xr.at[j])
        bcol = jnp.transpose(bbuf[j])
        keep = lax.broadcasted_iota(jnp.int32, (C, C), 1) <= lax.broadcasted_iota(jnp.int32, (C, C), 0)
        for r in range(R):
            row = min(r, R - 1 - r) * T
            col = 0 if r < R // 2 else C * (R - r)
            diag = wbuf[j, :, row : row + T, col + C * r : col + C * (r + 1)].reshape(C, C)
            diag = jnp.where(keep, diag, jnp.zeros_like(diag))
            acc = jnp.dot(diag, xin[j, r], preferred_element_type=jnp.float32)
            if r:
                before = wbuf[j, :, row : row + T, col : col + C * r].reshape(C, C * r)
                acc += jnp.dot(before, xin[j, :r].reshape(C * r, GD), preferred_element_type=jnp.float32)
            y[j, r] = (acc + bcol[:, r : r + 1]).astype(y.dtype)

        def give(r):
            ch = R * b + r
            sp, i = div(ch, NI), mod(ch, NI)
            dst = out.at[pl.ds(pl.multiple_of(i * C, C), C), pl.ds(pl.multiple_of(g * GD, GD), GD)]
            put(y.at[j, r], dst, ys, yr, sp, d)

        loop(R, give)

    last = hops

    def finish(jj):
        with jax.named_scope(f"partner{jj}"):
            arrived(wbuf.at[theirs[jj]], pr.at[jj])
            if jj == 0:
                arrived(bbuf, br)
        with jax.named_scope(f"compute{jj}"):
            loop(2, functools.partial(compute, jj))

    for b in range(NB // 2, NB):
        give_up(b)
    order = sorted((s + 1.4 * jj if s else jj - 0.5, jj, s) for jj in range(SH) for s in range(last + 1))
    pending = None
    for n, (_, jj, s) in enumerate(order):
        with jax.named_scope(f"ring{jj}_{s}"):
            ring(jj, s)
        if pending is not None:
            finish(pending)
            pending = None
        if s == last:
            pending = jj
        if n == len(order) - 3:
            with jax.named_scope("weights_gone"):
                weights_gone()
    finish(pending)
    with jax.named_scope("sends_gone"):
        loop(sent, lambda _: arrived(xin.at[0, 0], xs))
        loop(SH * (X - 1), lambda k: arrived(wbuf.at[0, 0], rs))
        loop(SH * X, lambda k: arrived(wbuf.at[0, 0], ps))
    with jax.named_scope("out_wait"):
        arrived(out, yr)
    with jax.named_scope("drain"):
        loop(sent, lambda _: arrived(y.at[0, 0], ys))


def mix(plan, value, w, mix_bias, norm_gain, norm_bias):
    hop = max(plan.HALF, 1)
    dma = pltpu.SemaphoreType.DMA
    anywhere, vmem = pl.BlockSpec(memory_space=pl.ANY), pl.BlockSpec(memory_space=pltpu.VMEM)
    unit = pltpu.VMEM((plan.S, plan.R, plan.C, GD), jnp.bfloat16)
    return pl.pallas_call(
        functools.partial(mixer, plan),
        out_shape=[jax.ShapeDtypeStruct(value.shape, value.dtype)] * 2,
        in_specs=[anywhere, anywhere, vmem, vmem, vmem],
        out_specs=[anywhere] * 2,
        scratch_shapes=[
            pltpu.VMEM(value.shape, value.dtype),
            pltpu.VMEM(value.shape, value.dtype),
            pltpu.VMEM((plan.R, plan.C), jnp.float32),
            pltpu.VMEM((plan.S, plan.X, plan.PR * plan.T, plan.PW), jnp.bfloat16),
            pltpu.VMEM((plan.PR * plan.T, plan.PW), jnp.bfloat16),
            unit, unit,
            pltpu.VMEM((plan.S, plan.R, plan.C), jnp.float32),
            dma, dma((plan.NI,)), dma, dma,
            pltpu.SemaphoreType.REGULAR((plan.far,)), pltpu.SemaphoreType.REGULAR((plan.NB,)),
            dma, dma((plan.SH,)), dma, dma, dma, dma((plan.S,)), dma,
            dma((plan.SH, hop)), dma((plan.SH, hop)), dma, dma((plan.SH,)), dma, dma,
        ],
        compiler_params=pltpu.CompilerParams(
            collective_id=0, has_side_effects=True, vmem_limit_bytes=60 * 1024 * 1024
        ),
    )(w, value, mix_bias, norm_gain, norm_bias)[0]


def body(sp, dp, gate_input, value_input, norm_gain, norm_bias, mix_weight, mix_bias):
    length, width = value_input.shape[1:]
    rows, blk = mix_weight.shape[1:]
    plan = Plan(sp, dp, length, width, rows, blk)
    mixed = mix(plan, value_input[0], mix_weight[0], mix_bias, norm_gain, norm_bias)
    gated = jax.nn.gelu(gate_input.astype(jnp.float32)) * mixed[None].astype(jnp.float32)
    return gated.astype(jnp.bfloat16)


def solution(mesh):
    placed = (
        P(("grp", "dp"), "sp", None),
        P(("grp", "dp"), "sp", None),
        P(),
        P(),
        P("sp", "dp", None),
        P("sp", None),
    )
    return jax.shard_map(
        functools.partial(body, mesh.shape["sp"], mesh.shape["dp"]),
        mesh=mesh, in_specs=placed, out_specs=P(("grp", "dp"), "sp", None), check_vma=False,
    )
```

```python
import functools

import jax
import jax.numpy as jnp
from jax import lax
from jax.experimental import pallas as pl
from jax.experimental.pallas import tpu as pltpu
from jax.sharding import PartitionSpec as P

GD = 128
BLK = 1024
MESH = pl.DeviceIdType.MESH


def div(a, n):
    if isinstance(a, int):
        return a // n
    if n & (n - 1) == 0:
        return lax.shift_right_logical(a, n.bit_length() - 1)
    return lax.shift_right_logical(a * (65536 // n + 1), 16)


def mod(a, n):
    if isinstance(a, int):
        return a % n
    return lax.bitwise_and(a, n - 1) if n & (n - 1) == 0 else a - n * div(a, n)


class Plan:
    def __init__(self, sp, dp, length, width, rows, blk):
        self.sp, self.dp = sp, dp
        self.X = dp // 2
        self.C = rows * 2
        self.R = blk // self.C
        self.NI = length // self.C
        self.NB = sp * length // blk
        self.G = width // GD
        self.S = self.NB * self.G // sp
        self.SH = self.S // 2
        self.T = self.C // self.X
        self.PR = self.R // 2
        self.PW = self.C * (self.R + 1)
        self.HALF = self.X // 2
        assert self.G % 5 and self.G & (self.G - 1) == 0
        far = 0
        for z in range(sp):
            for i in range(self.NI):
                for u in range(self.G):
                    far = max(far, abs((self.G * ((self.NI * z + i) // self.R) + u) // self.S - z))
        self.far = far

    def group(self, p):
        return div(p, self.G), mod(mod(p, self.G) * 5, self.G)

    def item(self, b, g):
        return self.G * b + mod(g * pow(5, -1, self.G), self.G)


def loop(n, body):
    def step(k, carry):
        body(k)
        return carry

    lax.fori_loop(0, n, step, 0)


def mixer(plan, w_hbm, value, mix_bias, norm_gain, norm_bias, out, normed, w, vbuf, nbuf, bias, wbuf, sblk, xin, y, bbuf, vs, ws, ns, l0s, l0r, rdn, rdw, w1s, w1r, bs, br, xs, xr, rs, rr, rl, ps, pr, ys, yr):
    X, C, R, NI, NB, G, S, SH, T, PR = (
        plan.X, plan.C, plan.R, plan.NI, plan.NB, plan.G, plan.S, plan.SH, plan.T, plan.PR,
    )
    z = lax.axis_index("sp")
    d = lax.axis_index("dp")
    x, c = div(d, 2), mod(d, 2)
    right = {"sp": z, "dp": 2 * mod(x + 1, X) + c}
    left = {"sp": z, "dp": 2 * mod(x + X - 1, X) + c}
    partner = {"sp": z, "dp": 2 * x + 1 - c}

    def remote(src, dst, send, recv, to):
        return pltpu.make_async_remote_copy(
            src_ref=src, dst_ref=dst, send_sem=send, recv_sem=recv, device_id=to, device_id_type=MESH
        )

    def put(src, dst, send, recv, sp, dp):
        here = jnp.logical_and(sp == z, dp == d)

        @pl.when(here)
        def _():
            pltpu.make_async_copy(src, dst, recv).start()

        @pl.when(jnp.logical_not(here))
        def _():
            remote(src, dst, send, recv, {"sp": sp, "dp": dp}).start()

    def arrived(ref, sem):
        pltpu.make_async_copy(ref, ref, sem).wait()

    def rows(k):
        return pl.ds(pl.multiple_of(k * C, C), C)

    load = pltpu.make_async_copy(value, vbuf, vs)
    load.start()
    load_w = pltpu.make_async_copy(w_hbm, w, ws)
    load_w.start()

    bar = pltpu.get_barrier_semaphore()

    def greet(sp, dp):
        pl.semaphore_signal(bar, inc=1, device_id={"sp": sp, "dp": dp}, device_id_type=MESH)

    def owner(b):
        return div(plan.item(b, z), S)

    def source(j):
        return plan.group(S * z + j)

    def greet_plane(k, n):
        dp = 2 * k + div(x, plan.HALF)
        pl.when(dp != d)(lambda: greet(z, dp))
        return n + (dp != d).astype(jnp.int32)

    def greet_owner(b, n):
        up = owner(b)
        pl.when(up > z)(lambda: greet(up, d))
        return n + (up < z).astype(jnp.int32)

    def greet_source(j, n):
        up = source(j)[1]
        pl.when(up > z)(lambda: greet(up, d))
        return n + (up < z).astype(jnp.int32)

    for to in (right, left, partner):
        pl.semaphore_signal(bar, inc=1, device_id=to, device_id_type=MESH)
    met = jnp.int32(3)
    for k in range(X):
        met = greet_plane(k, met)
    for far in range(1, plan.far + 1):
        pl.when(z + far < plan.sp)(functools.partial(greet, z + far, d))
        met += (z >= far).astype(jnp.int32)
    for b in range(NB):
        met = greet_owner(b, met)
    for j in range(S):
        met = greet_source(j, met)
    with jax.named_scope("barrier"):
        pl.semaphore_wait(bar, met)

    def plane_leg(k):
        ncol = C * (k + 1)
        row = min(k, R - 1 - k) * T
        col = 0 if k < R // 2 else C * (R - k)

        def strip(n):
            q, core = div(n, 2), mod(n, 2)
            put(
                w.at[pl.ds(pl.multiple_of(q * T, T), T), pl.ds(0, ncol)],
                sblk.at[pl.ds(row, T), pl.ds(col, ncol)],
                l0s, l0r, z, 2 * (plan.HALF * c + q) + core,
            )

        loop(2 * plan.HALF, strip)

    for r in range(R):
        bias[r : r + 1, :] = mix_bias[:, C * r : C * (r + 1)].astype(jnp.float32)

    load_w.wait()
    with jax.named_scope("plane_leg"):
        for k in range(X):
            pl.when(x == k)(functools.partial(plane_leg, k))

    def ready(j):
        b, g = source(j)

        @pl.when(g < z)
        def _():
            pl.semaphore_signal(rdw.at[b], inc=1, device_id={"sp": g, "dp": d}, device_id_type=MESH)

    loop(S, ready)
    for far in range(1, plan.far + 1):
        @pl.when(z >= far)
        def _(far=far):
            pl.semaphore_signal(rdn.at[far - 1], inc=1, device_id={"sp": z - far, "dp": d}, device_id_type=MESH)

    def give_weights(b):
        p = plan.item(b, z)
        j, own = mod(p, S), div(p, S)
        mine = div(j, SH) == c

        @pl.when(own == z)
        def _():
            pltpu.make_async_copy(bias, bbuf.at[j], br).start()

            @pl.when(mine)
            def _():
                wbuf[j, x] = sblk[...]

        @pl.when(own != z)
        def _():
            to = {"sp": own, "dp": d}
            remote(bias, bbuf.at[j], bs, br, to).start()

            @pl.when(mine)
            def _():
                remote(sblk, wbuf.at[j, x], w1s, w1r.at[mod(j, SH)], to).start()

    def give_down(b):
        pl.when(owner(b) <= z)(lambda: give_weights(b))

    def give_up(b):
        with jax.named_scope(f"give_up{b}"):
            @pl.when(owner(b) > z)
            def _():
                pl.semaphore_wait(rdw.at[b], 1)
                give_weights(b)

    def weights_gone():
        for k in range(X):
            @pl.when(x == k)
            def _(k=k):
                part = w.at[pl.ds(0, T), pl.ds(0, C * (k + 1))]
                own = (div(x, plan.HALF) == c).astype(jnp.int32)
                loop(2 * plan.HALF - own, lambda _: arrived(part, l0s))

        def one(b):
            @pl.when(owner(b) != z)
            def _():
                arrived(bias, bs)

                @pl.when(div(mod(plan.item(b, z), S), SH) == c)
                def _():
                    arrived(sblk, w1s)

        loop(NB, one)

    def normalize_all():
        step_rows = min(16, C)

        def normalize(k):
            at = pl.ds(pl.multiple_of(k * step_rows, step_rows), step_rows)
            act = jax.nn.gelu(vbuf[at, :].astype(jnp.float32))
            mean = jnp.mean(act, axis=-1, keepdims=True)
            act = act - mean
            var = jnp.mean(jnp.square(act), axis=-1, keepdims=True)
            nbuf[at, :] = (act * lax.rsqrt(var + 1e-06) * gain + shift).astype(nbuf.dtype)

        gain = norm_gain[...].astype(jnp.float32).reshape(1, G * GD)
        shift = norm_bias[...].astype(jnp.float32).reshape(1, G * GD)
        with jax.named_scope("normalize"):
            load.wait()
            for i in range(NI):
                def two(k, i=i):
                    normalize(i * (C // step_rows) + 2 * k)
                    normalize(i * (C // step_rows) + 2 * k + 1)

                loop(C // step_rows // 2, two)
                pltpu.make_async_copy(nbuf.at[rows(i)], normed.at[rows(i)], ns.at[i]).start()
            for i in range(NI):
                arrived(nbuf.at[rows(i)], ns.at[i])

    def send_units(wanted):
        def unit(k, n):
            i, g = div(k, G), mod(k, G)
            ch = NI * z + i
            b, r = div(ch, R), mod(ch, R)
            p = plan.item(b, g)
            own = div(p, S)

            @pl.when(wanted(own))
            def _():
                src = normed.at[rows(i), pl.ds(pl.multiple_of(g * GD, GD), GD)]
                put(src, xin.at[mod(p, S), r], xs, xr.at[mod(p, S)], own, d)

            return n

        lax.fori_loop(0, NI * G, unit, 0)

    def send_all_units():
        with jax.named_scope("units_down"):
            send_units(lambda own: own <= z)
        for far in range(1, plan.far + 1):
            with jax.named_scope(f"units_up{far}"):
                @pl.when(z + far < plan.sp)
                def _(far=far):
                    pl.semaphore_wait(rdn.at[far - 1], 1)
                    send_units(lambda own: own == z + far)

    normalize_all()
    with jax.named_scope("plane_wait"):
        arrived(sblk, l0r)
        loop(NB, give_down)
    for b in range(NB // 2):
        give_up(b)

    @pl.when(z >= plan.sp // 2)
    def _():
        for b in range(NB // 2, NB):
            give_up(b)

    def away(k, n):
        return n + (div(plan.item(div(NI * z + div(k, G), R), mod(k, G)), S) != z).astype(jnp.int32)

    sent = lax.fori_loop(0, NI * G, away, jnp.int32(0))

    hops = plan.HALF

    def ranked(core):
        groups = [source(SH * core + k)[1] for k in range(SH)]
        late = [jnp.where(g >= z, g, jnp.where(g == 0, 2 * plan.sp, 2 * z - g)) for g in groups]
        keys = [k + SH * g for k, g in enumerate(late)]
        ranks = [sum((a < b).astype(jnp.int32) for a in keys) for b in keys]
        return [SH * core + sum(k * (ranks[k] == n).astype(jnp.int32) for k in range(SH)) for n in range(SH)]

    mine, theirs = ranked(c), ranked(1 - c)

    half = PR * T // 2

    def part(jj, blk, h):
        return wbuf.at[mine[jj], blk, pl.ds(h * half, half)]

    def pass_on(jj, blk, h, send, recv, to):
        remote(part(jj, blk, h), part(jj, blk, h), send, recv, to).start()

    def ring(jj, s):
        more = mod(jj + c, 2) == 0
        if s == 0:
            @pl.when(source(mine[jj])[1] != z)
            def _():
                arrived(wbuf.at[mine[jj], x], w1r.at[mod(mine[jj], SH)])

        for h in range(2):
            for sems, to, blk, longer in (
                (rr, right, mod(x + X - s, X), more),
                (rl, left, mod(x + s, X), jnp.logical_not(more)),
            ):
                def step(forward, sems=sems, to=to, blk=blk, h=h):
                    if s:
                        arrived(part(jj, blk, h), sems.at[jj, 2 * s - 2 + h])
                    if forward is True:
                        pass_on(jj, blk, h, rs, sems.at[jj, 2 * s + h], to)
                    elif forward is not False:
                        @pl.when(forward)
                        def _():
                            pass_on(jj, blk, h, rs, sems.at[jj, 2 * s + h], to)
                    if s:
                        pass_on(jj, blk, h, ps, pr.at[jj], partner)

                if s < hops - 1:
                    step(True)
                elif s < hops:
                    step(longer)
                else:
                    pl.when(longer)(functools.partial(step, False))
            if s == 0:
                pass_on(jj, x, h, ps, pr.at[jj], partner)

    def compute(jj, other):
        j = theirs[jj] if other else mine[jj]
        b, g = plan.group(S * z + j)
        arrived(xin.at[j], xr.at[j])
        bcol = jnp.transpose(bbuf[j])
        keep = lax.broadcasted_iota(jnp.int32, (C, C), 1) <= lax.broadcasted_iota(jnp.int32, (C, C), 0)
        for r in range(R):
            row = min(r, R - 1 - r) * T
            col = 0 if r < R // 2 else C * (R - r)
            diag = wbuf[j, :, row : row + T, col + C * r : col + C * (r + 1)].reshape(C, C)
            diag = jnp.where(keep, diag, jnp.zeros_like(diag))
            acc = jnp.dot(diag, xin[j, r], preferred_element_type=jnp.float32)
            if r:
                before = wbuf[j, :, row : row + T, col : col + C * r].reshape(C, C * r)
                acc += jnp.dot(before, xin[j, :r].reshape(C * r, GD), preferred_element_type=jnp.float32)
            y[j, r] = (acc + bcol[:, r : r + 1]).astype(y.dtype)

        def give(r):
            ch = R * b + r
            sp, i = div(ch, NI), mod(ch, NI)
            dst = out.at[pl.ds(pl.multiple_of(i * C, C), C), pl.ds(pl.multiple_of(g * GD, GD), GD)]
            put(y.at[j, r], dst, ys, yr, sp, d)

        loop(R, give)

    last = hops

    def finish(jj, other):
        if other:
            with jax.named_scope(f"partner{jj}"):
                arrived(wbuf.at[theirs[jj]], pr.at[jj])
        elif jj == 0:
            arrived(bbuf, br)
        with jax.named_scope(f"compute{jj}_{other}"):
            compute(jj, other)

    order = sorted((s + 2.8 * jj, jj, s) for jj in range(SH) for s in range(last + 1))
    at = {}
    for b in range(NB // 2, NB):
        at.setdefault(min(b - NB // 2 + 1, len(order) - 1), []).append(b)
    own_first = source(mine[0])[1] == z
    pl.when(jnp.logical_not(own_first))(send_all_units)
    todo = []
    for n, (_, jj, s) in enumerate(order):
        with jax.named_scope(f"ring{jj}_{s}"):
            ring(jj, s)
        if n == 0:
            pl.when(own_first)(send_all_units)
        for b in at.get(n, []):
            pl.when(z < plan.sp // 2)(functools.partial(give_up, b))
        if todo and n >= len(order) - SH - 2:
            finish(*todo.pop(0))
        if s == last:
            todo += [(jj, 0), (jj, 1)]
        if n == len(order) - 3:
            with jax.named_scope("weights_gone"):
                weights_gone()
    for job in todo:
        finish(*job)
    with jax.named_scope("sends_gone"):
        loop(sent, lambda _: arrived(xin.at[0, 0], xs))
        loop(2 * SH * (X - 1), lambda k: arrived(wbuf.at[0, 0, pl.ds(0, half)], rs))
        loop(SH * X, lambda k: arrived(wbuf.at[0, 0], ps))
    with jax.named_scope("out_wait"):
        arrived(out, yr)
    with jax.named_scope("drain"):
        loop(sent, lambda _: arrived(y.at[0, 0], ys))


def mix(plan, value, w, mix_bias, norm_gain, norm_bias):
    hop = max(plan.HALF, 1)
    dma = pltpu.SemaphoreType.DMA
    anywhere, vmem = pl.BlockSpec(memory_space=pl.ANY), pl.BlockSpec(memory_space=pltpu.VMEM)
    unit = pltpu.VMEM((plan.S, plan.R, plan.C, GD), jnp.bfloat16)
    return pl.pallas_call(
        functools.partial(mixer, plan),
        out_shape=[jax.ShapeDtypeStruct(value.shape, value.dtype)] * 2,
        in_specs=[anywhere, anywhere, vmem, vmem, vmem],
        out_specs=[anywhere] * 2,
        scratch_shapes=[
            pltpu.VMEM(w.shape, w.dtype),
            pltpu.VMEM(value.shape, value.dtype),
            pltpu.VMEM(value.shape, value.dtype),
            pltpu.VMEM((plan.R, plan.C), jnp.float32),
            pltpu.VMEM((plan.S, plan.X, plan.PR * plan.T, plan.PW), jnp.bfloat16),
            pltpu.VMEM((plan.PR * plan.T, plan.PW), jnp.bfloat16),
            unit, unit,
            pltpu.VMEM((plan.S, plan.R, plan.C), jnp.float32),
            dma, dma, dma((plan.NI,)), dma, dma,
            pltpu.SemaphoreType.REGULAR((plan.far,)), pltpu.SemaphoreType.REGULAR((plan.NB,)),
            dma, dma((plan.SH,)), dma, dma, dma, dma((plan.S,)), dma,
            dma((plan.SH, 2 * hop)), dma((plan.SH, 2 * hop)), dma, dma((plan.SH,)), dma, dma,
        ],
        compiler_params=pltpu.CompilerParams(
            collective_id=0, has_side_effects=True, vmem_limit_bytes=60 * 1024 * 1024
        ),
    )(w, value, mix_bias, norm_gain, norm_bias)[0]


def body(sp, dp, gate_input, value_input, norm_gain, norm_bias, mix_weight, mix_bias):
    length, width = value_input.shape[1:]
    rows, blk = mix_weight.shape[1:]
    plan = Plan(sp, dp, length, width, rows, blk)
    mixed = mix(plan, value_input[0], mix_weight[0], mix_bias, norm_gain, norm_bias)
    gated = jax.nn.gelu(gate_input.astype(jnp.float32)) * mixed[None].astype(jnp.float32)
    return gated.astype(jnp.bfloat16)


def solution(mesh):
    placed = (
        P(("grp", "dp"), "sp", None),
        P(("grp", "dp"), "sp", None),
        P(),
        P(),
        P("sp", "dp", None),
        P("sp", None),
    )
    return jax.shard_map(
        functools.partial(body, mesh.shape["sp"], mesh.shape["dp"]),
        mesh=mesh, in_specs=placed, out_specs=P(("grp", "dp"), "sp", None), check_vma=False,
    )
```

```python
import functools

import jax
import jax.numpy as jnp
from jax import lax
from jax.experimental import pallas as pl
from jax.experimental.pallas import tpu as pltpu
from jax.sharding import PartitionSpec as P

GD = 128
BLK = 1024
MESH = pl.DeviceIdType.MESH


def div(a, n):
    if isinstance(a, int):
        return a // n
    if n & (n - 1) == 0:
        return lax.shift_right_logical(a, n.bit_length() - 1)
    return lax.shift_right_logical(a * (65536 // n + 1), 16)


def mod(a, n):
    if isinstance(a, int):
        return a % n
    return lax.bitwise_and(a, n - 1) if n & (n - 1) == 0 else a - n * div(a, n)


class Plan:
    def __init__(self, sp, dp, length, width, rows, blk):
        self.sp, self.dp = sp, dp
        self.X = dp // 2
        self.C = rows * 2
        self.R = blk // self.C
        self.NI = length // self.C
        self.NB = sp * length // blk
        self.G = width // GD
        self.S = self.NB * self.G // sp
        self.SH = self.S // 2
        self.T = self.C // self.X
        self.PR = self.R // 2
        self.PW = self.C * (self.R + 1)
        self.HALF = self.X // 2
        assert self.G % 3 and self.G & (self.G - 1) == 0
        far = 0
        for z in range(sp):
            for i in range(self.NI):
                for u in range(self.G):
                    far = max(far, abs((self.G * ((self.NI * z + i) // self.R) + u) // self.S - z))
        self.far = far

    def group(self, p):
        return div(p, self.G), mod(mod(p, self.G) * 3, self.G)

    def item(self, b, g):
        return self.G * b + mod(g * pow(3, -1, self.G), self.G)


def loop(n, body):
    def step(k, carry):
        body(k)
        return carry

    lax.fori_loop(0, n, step, 0)


def mixer(plan, w_hbm, value, mix_bias, norm_gain, norm_bias, out, normed, w, vbuf, nbuf, bias, wbuf, sblk, xin, y, bbuf, vs, ws, ns, l0s, l0r, rdn, rdw, w1s, w1r, bs, br, xs, xr, rs, rr, rl, ps, pr, ys, yr):
    X, C, R, NI, NB, G, S, SH, T, PR = (
        plan.X, plan.C, plan.R, plan.NI, plan.NB, plan.G, plan.S, plan.SH, plan.T, plan.PR,
    )
    z = lax.axis_index("sp")
    d = lax.axis_index("dp")
    x, c = div(d, 2), mod(d, 2)
    right = {"sp": z, "dp": 2 * mod(x + 1, X) + c}
    left = {"sp": z, "dp": 2 * mod(x + X - 1, X) + c}
    partner = {"sp": z, "dp": 2 * x + 1 - c}

    def remote(src, dst, send, recv, to):
        return pltpu.make_async_remote_copy(
            src_ref=src, dst_ref=dst, send_sem=send, recv_sem=recv, device_id=to, device_id_type=MESH
        )

    def put(src, dst, send, recv, sp, dp):
        here = jnp.logical_and(sp == z, dp == d)

        @pl.when(here)
        def _():
            pltpu.make_async_copy(src, dst, recv).start()

        @pl.when(jnp.logical_not(here))
        def _():
            remote(src, dst, send, recv, {"sp": sp, "dp": dp}).start()

    def arrived(ref, sem):
        pltpu.make_async_copy(ref, ref, sem).wait()

    def rows(k):
        return pl.ds(pl.multiple_of(k * C, C), C)

    load = pltpu.make_async_copy(value, vbuf, vs)
    load.start()
    load_w = pltpu.make_async_copy(w_hbm, w, ws)
    load_w.start()

    bar = pltpu.get_barrier_semaphore()

    def greet(sp, dp):
        pl.semaphore_signal(bar, inc=1, device_id={"sp": sp, "dp": dp}, device_id_type=MESH)

    def owner(b):
        return div(plan.item(b, z), S)

    def source(j):
        return plan.group(S * z + j)

    def greet_plane(k, n):
        dp = 2 * k + div(x, plan.HALF)
        pl.when(dp != d)(lambda: greet(z, dp))
        return n + (dp != d).astype(jnp.int32)

    def greet_owner(b, n):
        up = owner(b)
        pl.when(up > z)(lambda: greet(up, d))
        return n + (up < z).astype(jnp.int32)

    def greet_source(j, n):
        up = source(j)[1]
        pl.when(up > z)(lambda: greet(up, d))
        return n + (up < z).astype(jnp.int32)

    for to in (right, left, partner):
        pl.semaphore_signal(bar, inc=1, device_id=to, device_id_type=MESH)
    met = jnp.int32(3)
    for k in range(X):
        met = greet_plane(k, met)
    for far in range(1, plan.far + 1):
        pl.when(z + far < plan.sp)(functools.partial(greet, z + far, d))
        met += (z >= far).astype(jnp.int32)
    for b in range(NB):
        met = greet_owner(b, met)
    for j in range(S):
        met = greet_source(j, met)
    with jax.named_scope("barrier"):
        pl.semaphore_wait(bar, met)

    def plane_leg(k):
        ncol = C * (k + 1)
        row = min(k, R - 1 - k) * T
        col = 0 if k < R // 2 else C * (R - k)

        def strip(n):
            q, core = div(n, 2), mod(n, 2)
            put(
                w.at[pl.ds(pl.multiple_of(q * T, T), T), pl.ds(0, ncol)],
                sblk.at[pl.ds(row, T), pl.ds(col, ncol)],
                l0s, l0r, z, 2 * (plan.HALF * c + q) + core,
            )

        loop(2 * plan.HALF, strip)

    for r in range(R):
        bias[r : r + 1, :] = mix_bias[:, C * r : C * (r + 1)].astype(jnp.float32)

    load_w.wait()
    with jax.named_scope("plane_leg"):
        for k in range(X):
            pl.when(x == k)(functools.partial(plane_leg, k))

    def ready(j):
        b, g = source(j)

        @pl.when(g < z)
        def _():
            pl.semaphore_signal(rdw.at[b], inc=1, device_id={"sp": g, "dp": d}, device_id_type=MESH)

    loop(S, ready)
    for far in range(1, plan.far + 1):
        @pl.when(z >= far)
        def _(far=far):
            pl.semaphore_signal(rdn.at[far - 1], inc=1, device_id={"sp": z - far, "dp": d}, device_id_type=MESH)

    def give_weights(b):
        p = plan.item(b, z)
        j, own = mod(p, S), div(p, S)
        mine = div(j, SH) == c

        @pl.when(own == z)
        def _():
            pltpu.make_async_copy(bias, bbuf.at[j], br).start()

            @pl.when(mine)
            def _():
                wbuf[j, x] = sblk[...]

        @pl.when(own != z)
        def _():
            to = {"sp": own, "dp": d}
            remote(bias, bbuf.at[j], bs, br, to).start()

            @pl.when(mine)
            def _():
                remote(sblk, wbuf.at[j, x], w1s, w1r.at[mod(j, SH)], to).start()

    def give_down(b):
        pl.when(owner(b) <= z)(lambda: give_weights(b))

    def give_up(b):
        with jax.named_scope(f"give_up{b}"):
            @pl.when(owner(b) > z)
            def _():
                pl.semaphore_wait(rdw.at[b], 1)
                give_weights(b)

    def weights_gone():
        for k in range(X):
            @pl.when(x == k)
            def _(k=k):
                part = w.at[pl.ds(0, T), pl.ds(0, C * (k + 1))]
                own = (div(x, plan.HALF) == c).astype(jnp.int32)
                loop(2 * plan.HALF - own, lambda _: arrived(part, l0s))

        def one(b):
            @pl.when(owner(b) != z)
            def _():
                arrived(bias, bs)

                @pl.when(div(mod(plan.item(b, z), S), SH) == c)
                def _():
                    arrived(sblk, w1s)

        loop(NB, one)

    def normalize_all():
        step_rows = min(16, C)

        def normalize(k):
            at = pl.ds(pl.multiple_of(k * step_rows, step_rows), step_rows)
            act = jax.nn.gelu(vbuf[at, :].astype(jnp.float32))
            mean = jnp.mean(act, axis=-1, keepdims=True)
            act = act - mean
            var = jnp.mean(jnp.square(act), axis=-1, keepdims=True)
            nbuf[at, :] = (act * lax.rsqrt(var + 1e-06) * gain + shift).astype(nbuf.dtype)

        gain = norm_gain[...].astype(jnp.float32).reshape(1, G * GD)
        shift = norm_bias[...].astype(jnp.float32).reshape(1, G * GD)
        with jax.named_scope("normalize"):
            load.wait()
            for i in range(NI):
                def two(k, i=i):
                    normalize(i * (C // step_rows) + 2 * k)
                    normalize(i * (C // step_rows) + 2 * k + 1)

                loop(C // step_rows // 2, two)
                pltpu.make_async_copy(nbuf.at[rows(i)], normed.at[rows(i)], ns.at[i]).start()
            for i in range(NI):
                arrived(nbuf.at[rows(i)], ns.at[i])

    def send_units(wanted):
        def unit(k, n):
            i, g = div(k, G), mod(k, G)
            ch = NI * z + i
            b, r = div(ch, R), mod(ch, R)
            p = plan.item(b, g)
            own = div(p, S)

            @pl.when(wanted(own))
            def _():
                src = normed.at[rows(i), pl.ds(pl.multiple_of(g * GD, GD), GD)]
                put(src, xin.at[mod(p, S), r], xs, xr.at[mod(p, S)], own, d)

            return n

        lax.fori_loop(0, NI * G, unit, 0)

    def send_all_units():
        with jax.named_scope("units_down"):
            send_units(lambda own: own <= z)
        for far in range(1, plan.far + 1):
            with jax.named_scope(f"units_up{far}"):
                @pl.when(z + far < plan.sp)
                def _(far=far):
                    pl.semaphore_wait(rdn.at[far - 1], 1)
                    send_units(lambda own: own == z + far)

    normalize_all()
    with jax.named_scope("plane_wait"):
        arrived(sblk, l0r)
        loop(NB, give_down)
    for b in range(NB // 2):
        give_up(b)

    @pl.when(z >= plan.sp // 2)
    def _():
        for b in range(NB // 2, NB):
            give_up(b)

    def away(k, n):
        return n + (div(plan.item(div(NI * z + div(k, G), R), mod(k, G)), S) != z).astype(jnp.int32)

    sent = lax.fori_loop(0, NI * G, away, jnp.int32(0))

    hops = plan.HALF

    def ranked(core):
        groups = [source(SH * core + k)[1] for k in range(SH)]
        late = [jnp.where(g >= z, g, jnp.where(g == 0, 2 * plan.sp, 2 * z - g)) for g in groups]
        keys = [k + SH * g for k, g in enumerate(late)]
        ranks = [sum((a < b).astype(jnp.int32) for a in keys) for b in keys]
        return [SH * core + sum(k * (ranks[k] == n).astype(jnp.int32) for k in range(SH)) for n in range(SH)]

    mine, theirs = ranked(c), ranked(1 - c)

    half = PR * T // 2

    def part(jj, blk, h):
        return wbuf.at[mine[jj], blk, pl.ds(h * half, half)]

    def pass_on(jj, blk, h, send, recv, to):
        remote(part(jj, blk, h), part(jj, blk, h), send, recv, to).start()

    def ring(jj, s):
        more = mod(jj + c, 2) == 0
        if s == 0:
            @pl.when(source(mine[jj])[1] != z)
            def _():
                arrived(wbuf.at[mine[jj], x], w1r.at[mod(mine[jj], SH)])

        for h in range(2):
            for sems, to, blk, longer in (
                (rr, right, mod(x + X - s, X), more),
                (rl, left, mod(x + s, X), jnp.logical_not(more)),
            ):
                def step(forward, sems=sems, to=to, blk=blk, h=h):
                    if s:
                        arrived(part(jj, blk, h), sems.at[jj, 2 * s - 2 + h])
                    if forward is True:
                        pass_on(jj, blk, h, rs, sems.at[jj, 2 * s + h], to)
                    elif forward is not False:
                        @pl.when(forward)
                        def _():
                            pass_on(jj, blk, h, rs, sems.at[jj, 2 * s + h], to)
                    if s:
                        pass_on(jj, blk, h, ps, pr.at[jj], partner)

                if s < hops - 1:
                    step(True)
                elif s < hops:
                    step(longer)
                else:
                    pl.when(longer)(functools.partial(step, False))
            if s == 0:
                pass_on(jj, x, h, ps, pr.at[jj], partner)

    def compute(jj, other):
        j = theirs[jj] if other else mine[jj]
        b, g = plan.group(S * z + j)
        arrived(xin.at[j], xr.at[j])
        bcol = jnp.transpose(bbuf[j])
        keep = lax.broadcasted_iota(jnp.int32, (C, C), 1) <= lax.broadcasted_iota(jnp.int32, (C, C), 0)
        for r in range(R):
            row = min(r, R - 1 - r) * T
            col = 0 if r < R // 2 else C * (R - r)
            diag = wbuf[j, :, row : row + T, col + C * r : col + C * (r + 1)].reshape(C, C)
            diag = jnp.where(keep, diag, jnp.zeros_like(diag))
            acc = jnp.dot(diag, xin[j, r], preferred_element_type=jnp.float32)
            if r:
                before = wbuf[j, :, row : row + T, col : col + C * r].reshape(C, C * r)
                acc += jnp.dot(before, xin[j, :r].reshape(C * r, GD), preferred_element_type=jnp.float32)
            y[j, r] = (acc + bcol[:, r : r + 1]).astype(y.dtype)

        def give(r):
            ch = R * b + r
            sp, i = div(ch, NI), mod(ch, NI)
            dst = out.at[pl.ds(pl.multiple_of(i * C, C), C), pl.ds(pl.multiple_of(g * GD, GD), GD)]
            put(y.at[j, r], dst, ys, yr, sp, d)

        loop(R, give)

    last = hops

    def finish(jj, other):
        if other:
            with jax.named_scope(f"partner{jj}"):
                arrived(wbuf.at[theirs[jj]], pr.at[jj])
        elif jj == 0:
            arrived(bbuf, br)
        with jax.named_scope(f"compute{jj}_{other}"):
            compute(jj, other)

    order = sorted((s + 2.8 * jj, jj, s) for jj in range(SH) for s in range(last + 1))
    at = {}
    for b in range(NB // 2, NB):
        at.setdefault(min(b - NB // 2 + 1, len(order) - 1), []).append(b)
    own_first = source(mine[0])[1] == z
    pl.when(jnp.logical_not(own_first))(send_all_units)
    todo = []
    for n, (_, jj, s) in enumerate(order):
        with jax.named_scope(f"ring{jj}_{s}"):
            ring(jj, s)
        if n == 0:
            pl.when(own_first)(send_all_units)
        for b in at.get(n, []):
            pl.when(z < plan.sp // 2)(functools.partial(give_up, b))
        if todo and n >= len(order) - SH - 2:
            finish(*todo.pop(0))
        if s == last:
            todo += [(jj, 0), (jj, 1)]
        if n == len(order) - 3:
            with jax.named_scope("weights_gone"):
                weights_gone()
    for job in todo:
        finish(*job)
    with jax.named_scope("sends_gone"):
        loop(sent, lambda _: arrived(xin.at[0, 0], xs))
        loop(2 * SH * (X - 1), lambda k: arrived(wbuf.at[0, 0, pl.ds(0, half)], rs))
        loop(SH * X, lambda k: arrived(wbuf.at[0, 0], ps))
    with jax.named_scope("out_wait"):
        arrived(out, yr)
    with jax.named_scope("drain"):
        loop(sent, lambda _: arrived(y.at[0, 0], ys))


def mix(plan, value, w, mix_bias, norm_gain, norm_bias):
    hop = max(plan.HALF, 1)
    dma = pltpu.SemaphoreType.DMA
    anywhere, vmem = pl.BlockSpec(memory_space=pl.ANY), pl.BlockSpec(memory_space=pltpu.VMEM)
    unit = pltpu.VMEM((plan.S, plan.R, plan.C, GD), jnp.bfloat16)
    return pl.pallas_call(
        functools.partial(mixer, plan),
        out_shape=[jax.ShapeDtypeStruct(value.shape, value.dtype)] * 2,
        in_specs=[anywhere, anywhere, vmem, vmem, vmem],
        out_specs=[anywhere] * 2,
        scratch_shapes=[
            pltpu.VMEM(w.shape, w.dtype),
            pltpu.VMEM(value.shape, value.dtype),
            pltpu.VMEM(value.shape, value.dtype),
            pltpu.VMEM((plan.R, plan.C), jnp.float32),
            pltpu.VMEM((plan.S, plan.X, plan.PR * plan.T, plan.PW), jnp.bfloat16),
            pltpu.VMEM((plan.PR * plan.T, plan.PW), jnp.bfloat16),
            unit, unit,
            pltpu.VMEM((plan.S, plan.R, plan.C), jnp.float32),
            dma, dma, dma((plan.NI,)), dma, dma,
            pltpu.SemaphoreType.REGULAR((plan.far,)), pltpu.SemaphoreType.REGULAR((plan.NB,)),
            dma, dma((plan.SH,)), dma, dma, dma, dma((plan.S,)), dma,
            dma((plan.SH, 2 * hop)), dma((plan.SH, 2 * hop)), dma, dma((plan.SH,)), dma, dma,
        ],
        compiler_params=pltpu.CompilerParams(
            collective_id=0, has_side_effects=True, vmem_limit_bytes=60 * 1024 * 1024
        ),
    )(w, value, mix_bias, norm_gain, norm_bias)[0]


def body(sp, dp, gate_input, value_input, norm_gain, norm_bias, mix_weight, mix_bias):
    length, width = value_input.shape[1:]
    rows, blk = mix_weight.shape[1:]
    plan = Plan(sp, dp, length, width, rows, blk)
    mixed = mix(plan, value_input[0], mix_weight[0], mix_bias, norm_gain, norm_bias)
    gated = jax.nn.gelu(gate_input.astype(jnp.float32)) * mixed[None].astype(jnp.float32)
    return gated.astype(jnp.bfloat16)


def solution(mesh):
    placed = (
        P(("grp", "dp"), "sp", None),
        P(("grp", "dp"), "sp", None),
        P(),
        P(),
        P("sp", "dp", None),
        P("sp", None),
    )
    return jax.shard_map(
        functools.partial(body, mesh.shape["sp"], mesh.shape["dp"]),
        mesh=mesh, in_specs=placed, out_specs=P(("grp", "dp"), "sp", None), check_vma=False,
    )
```
